32 devices in a mesh: ep: 8 (over z, x), tp: 4 (over y, core).
Axes of the slice: x: 2, y: 2, z: 4, core: 2. Of those that a mesh axis runs over, the one named last changes fastest.
Arguments:
- pool_input: bfloat16 [2048, 2048], P('ep', 'tp'), may hold values from -6 to 6
- pool_map: bfloat16 [16, 128, 128], replicated, may hold values from -0.5 to 0.5
- pool_scale: float32 [2048], replicated, may hold values from 0.1 to 1.9
- out_proj: bfloat16 [2048, 4096], P('tp'), may hold values from -0.125 to 0.125
- moe_input: bfloat16 [1024, 4096], P('ep'), may hold values from -6 to 6
- norm_gain: float32 [4096], replicated, may hold values from 0.1 to 1.9
- routes: int32 [1024, 4], P('ep'), may hold values from 0 to 7, all different within a row; in each aligned block of 128 rows (0 to 127, 128 to 255, ...) at most 96 rows name the same one
- route_weights: float32 [1024, 4], P('ep'), may hold values from 0.1 to 1
- expert_gate: bfloat16 [8, 4096, 1024], P('ep', None, 'tp'), may hold values from -0.09375 to 0.09375
- expert_up: bfloat16 [8, 4096, 1024], P('ep', None, 'tp'), may hold values from -0.09375 to 0.09375
- expert_down: bfloat16 [8, 1024, 4096], P('ep', None, 'tp'), may hold values from -0.1875 to 0.1875
- shared_gate: bfloat16 [4096, 512], P(None, 'tp'), may hold values from -0.09375 to 0.09375
- shared_up: bfloat16 [4096, 512], P(None, 'tp'), may hold values from -0.09375 to 0.09375
- shared_down: bfloat16 [512, 4096], P('tp'), may hold values from -0.25 to 0.25
Outputs:
- mixer_output: bfloat16 [2048, 4096], P('ep', 'tp')
- moe_output: bfloat16 [1024, 4096], P('ep', 'tp')
The draws below stay inside these ranges and needn't reach their ends.
Inputs may be any that keep to these rules, and one draw needn't show every extreme that they name: `routes`: each row names 4 different experts. In each aligned block of 128 rows no expert is named by more than 96 rows, a bound that some block reaches.
All inputs are finite; a program needn't handle non-finite values.
Results may differ from the reference program's by a relative error of at most 0.017.
Values may be sent and summed in bfloat16 or wider, within the bound.
A program may use at most 64 MiB of HBM per device.

```python
import math
import jax
import jax.numpy as jnp
import numpy as np
from jax import lax

D = 4096
POOL_WIDTH = 2048
POOL_GROUPS = 16
GROUP_DIM = 128
EXPERT_DIM = 1024
SHARED_DIM = 512
TOP_K = 4
TOK2_DEV = 128
TOK1 = 2048
TOK2 = 1024
EXPERTS = 8
CAP = 96
EXPERT_ROWS = 768
N_EP = 8
N_TP = 4


def level_of(key, extent, pieces, smallest, largest):
    gain, own = 1.0, jax.random.fold_in(key, 6)
    for dim, blocks in pieces:
        steps = jnp.exp(jax.random.uniform(jax.random.fold_in(own, dim), (blocks,), jnp.float32, smallest / len(pieces), largest / len(pieces)))
        gain = gain * jnp.repeat(steps, extent[dim] // blocks).reshape([-1 if axis == dim else 1 for axis in range(len(extent))])
    return gain


def routed_block(own_key, own, number, rows, number_of, top, reach, lean):
    ranking = jax.random.permutation(own_key, number_of)
    heavy_load, common = load_shares(number_of, rows * top, reach, lean, True), load_shares(number_of, rows * top, reach, lean, False)
    places = jnp.arange(number_of)

    def named(lengths, offset_by):
        used = int((lengths > 0).sum())
        fixed = max(1, used // 4)
        shifted = fixed + (places - fixed + offset_by * (used - fixed)) % max(1, number_of - fixed)
        return jnp.zeros((number_of,), jnp.int32).at[ranking[jnp.where(places < fixed, places, shifted)]].set(jnp.asarray(lengths, jnp.int32))

    lengths = jnp.where(number % 4 == 0, named(heavy_load, number // 4), named(common, number - number // 4 - 1))
    mixed = jax.random.permutation(jax.random.fold_in(own, 3), number_of)
    giver, receiver = mixed[0:number_of // 2 * 2:2], mixed[1:number_of // 2 * 2:2]
    margin = jnp.minimum(lengths[giver] - 1, reach - lengths[receiver]) // 2
    margin = jnp.where((giver == ranking[0]) | (receiver == ranking[0]) | (lengths[receiver] == 0), 0, jnp.maximum(margin, 0))
    shifted = jax.random.randint(jax.random.fold_in(own, 4), (number_of // 2,), 0, 1 << 20) % (margin + 1)
    lengths = lengths.at[giver].add(-shifted).at[receiver].add(shifted)
    members = jnp.searchsorted(jnp.cumsum(lengths), jnp.arange(rows * top), side="right").astype(jnp.int32)
    grid = members.reshape(top, rows).T
    grid = grid[jax.random.permutation(jax.random.fold_in(own, 1), rows)]
    offset_by = jax.random.randint(jax.random.fold_in(own, 2), (rows, 1), 0, top)
    return jnp.take_along_axis(grid, (jnp.arange(top)[None, :] + offset_by) % top, axis=1)


def load_shares(amount, total, limit, slope, full):
    loads = [(1 << 20) // math.isqrt(rank ** slope) + 1 for rank in range(1, amount + 1)]
    largest = limit if full else min(limit, max(-(-total // amount), total * loads[0] // sum(loads)))
    least = 1 if total - largest >= amount - 1 else 0
    given, spare = [largest] + [least] * (amount - 1), total - largest - least * (amount - 1)
    while spare > 0:
        candidates = [i for i in range(1, amount) if given[i] < largest] or [i for i in range(1, amount) if given[i] < limit]
        whole, left = sum([loads[i] for i in candidates]), spare
        for i in candidates:
            addition = min(limit - given[i], max(1, left * loads[i] // whole), spare)
            given[i] = given[i] + addition
            spare = spare - addition
    return np.array(given)


def bell_draw(key, shape, spread, reach, shards=(), kind=jnp.bfloat16):
    entries = jax.random.normal(key, shape, jnp.float32) * spread
    if len(shards) > 0:
        entries = level_of(key, shape, shards, -0.22, 0.18) * entries
    return jnp.clip(entries, min=-reach, max=reach).astype(kind)


def setup_inputs(seed: int = 0) -> dict:
    arg_keys = jax.random.split(jax.random.key(seed), 15)
    pool_input = bell_draw(arg_keys[0], (TOK1, POOL_WIDTH), 1.0, 6.0, ((0, 8), (1, 4)))
    pool_map = bell_draw(arg_keys[1], (POOL_GROUPS, GROUP_DIM, GROUP_DIM), GROUP_DIM ** -0.5, 0.5)
    pool_scale = jnp.clip(1.0 + 0.18 * jax.random.normal(arg_keys[2], (POOL_WIDTH,), jnp.float32), 0.1, 1.9)
    out_proj = bell_draw(arg_keys[3], (POOL_WIDTH, D), POOL_WIDTH ** -0.5, 0.125, ((0, 4),))
    moe_input = bell_draw(arg_keys[4], (TOK2, D), 1.0, 6.0, ((0, 8),))
    norm_gain = jnp.clip(1.0 + 0.18 * jax.random.normal(arg_keys[5], (D,), jnp.float32), 0.1, 1.9)
    routes_keys = jax.random.split(jax.random.fold_in(arg_keys[6], 1), TOK2 // TOK2_DEV)
    routes_turns = jax.random.permutation(jax.random.fold_in(arg_keys[6], 3), TOK2 // TOK2_DEV)
    routes = jax.vmap(lambda own, number: routed_block(jax.random.fold_in(arg_keys[6], 2), own, number, TOK2_DEV, EXPERTS, TOP_K, CAP, 1))(routes_keys, routes_turns).reshape((TOK2, TOP_K))
    route_weights = jnp.clip(jnp.exp(math.log(1.0) - 2.3025851 * jax.random.uniform(arg_keys[7], (TOK2, TOP_K), jnp.float32) ** level_of(arg_keys[7], (TOK2, TOP_K), ((0, 8),), -0.2, 0.2)), 0.1, 1.0)
    expert_gate = bell_draw(arg_keys[8], (EXPERTS, D, EXPERT_DIM), D ** -0.5, 0.09375, ((0, 8), (2, 4)))
    expert_up = bell_draw(arg_keys[9], (EXPERTS, D, EXPERT_DIM), D ** -0.5, 0.09375, ((0, 8), (2, 4)))
    expert_down = bell_draw(arg_keys[10], (EXPERTS, EXPERT_DIM, D), EXPERT_DIM ** -0.5, 0.1875, ((0, 8), (2, 4)))
    shared_gate = bell_draw(arg_keys[11], (D, SHARED_DIM), D ** -0.5, 0.09375, ((1, 4),))
    shared_up = bell_draw(arg_keys[12], (D, SHARED_DIM), D ** -0.5, 0.09375, ((1, 4),))
    shared_down = bell_draw(arg_keys[13], (SHARED_DIM, D), SHARED_DIM ** -0.5, 0.25, ((0, 4),))
    return {"pool_input": pool_input, "pool_map": pool_map, "pool_scale": pool_scale, "out_proj": out_proj, "moe_input": moe_input, "norm_gain": norm_gain, "routes": routes, "route_weights": route_weights, "expert_gate": expert_gate, "expert_up": expert_up, "expert_down": expert_down, "shared_gate": shared_gate, "shared_up": shared_up, "shared_down": shared_down}


windows = (2, 4, 8, 16)
reach_back = 15
eps = 1e-05

def pool_mixer(pool_input, pool_map, pool_scale, out_proj):
    row_count = pool_input.shape[0]
    channels = pool_input.shape[1]
    values = pool_input.astype(jnp.float32)
    padded = jnp.concatenate([jnp.zeros((reach_back, channels), jnp.float32), values], axis=0)
    position = jnp.arange(row_count, dtype=jnp.float32)
    group_kind = jnp.arange(channels, dtype=jnp.int32) // GROUP_DIM % 4
    running = jnp.zeros((row_count, channels), jnp.float32)
    pooled = -values
    for lag_step in range(reach_back + 1):
        running = running + padded[reach_back - lag_step:reach_back - lag_step + row_count]
        if lag_step + 1 in windows:
            kind_id = windows.index(lag_step + 1)
            counts = jnp.minimum(position + 1.0, float(lag_step + 1))
            select = (group_kind == kind_id).astype(jnp.float32)
            pooled = pooled + select[None, :] * running / counts[:, None]
    pooled = pooled.astype(jnp.bfloat16)
    grouped = pooled.reshape(row_count, POOL_GROUPS, GROUP_DIM).astype(jnp.float32)
    mapped = jnp.einsum('rgc,gcd->rgd', grouped, pool_map.astype(jnp.float32)).reshape(row_count, channels)
    group_out = (mapped * pool_scale[None, :]).astype(jnp.bfloat16)
    block_width = channels // N_TP
    mixed = jnp.zeros((row_count, out_proj.shape[1]), jnp.float32)
    for block_idx in range(N_TP):
        lower = block_idx * block_width
        partial_sum = jnp.dot(group_out[:, lower:lower + block_width], out_proj[lower:lower + block_width], preferred_element_type=jnp.float32).astype(jnp.bfloat16)
        partial_sum = lax.optimization_barrier(partial_sum)
        mixed = mixed + partial_sum.astype(jnp.float32)
    return mixed.astype(jnp.bfloat16)

def slot_rows(routes):
    blocks = routes.reshape(N_EP, TOK2_DEV * TOP_K)
    one_hot = (blocks[:, :, None] == jnp.arange(EXPERTS, dtype=jnp.int32)[None, None, :]).astype(jnp.int32)
    earlier = jnp.cumsum(one_hot, axis=1) - one_hot
    slot_ids = lax.optimization_barrier(jnp.sum(earlier * one_hot, axis=2))
    block_ids = jnp.arange(N_EP, dtype=jnp.int32)[:, None]
    buffer_row = blocks * EXPERT_ROWS + block_ids * CAP + slot_ids
    return buffer_row.reshape(TOK2, TOP_K).astype(jnp.int32)

def one_expert(operands):
    rows_in, gate_weight, up_weight, down_weight = operands
    gate_val = jnp.dot(rows_in, gate_weight, preferred_element_type=jnp.float32)
    up_val = jnp.dot(rows_in, up_weight, preferred_element_type=jnp.float32)
    hidden = (jax.nn.silu(gate_val) * up_val).astype(jnp.bfloat16)
    return jnp.dot(hidden, down_weight, preferred_element_type=jnp.float32).astype(jnp.bfloat16)

def moe_layer(moe_input, norm_gain, routes, route_weights, expert_gate, expert_up, expert_down, shared_gate, shared_up, shared_down):
    values = moe_input.astype(jnp.float32)
    centre = values - lax.optimization_barrier(jnp.mean(values, axis=1, keepdims=True))
    variance = lax.optimization_barrier(jnp.mean(centre * centre, axis=1, keepdims=True))
    normed = (centre * lax.rsqrt(variance + eps) * norm_gain[None, :]).astype(jnp.bfloat16)
    buffer_row = slot_rows(routes)
    repeated = jnp.repeat(normed, TOP_K, axis=0)
    buffers = jnp.zeros((EXPERTS * EXPERT_ROWS, D), jnp.bfloat16).at[buffer_row.reshape(-1)].set(repeated)
    buffers = buffers.reshape(EXPERTS, EXPERT_ROWS, D)
    expert_out = lax.map(one_expert, (buffers, expert_gate, expert_up, expert_down))
    expert_out = expert_out.reshape(EXPERTS * EXPERT_ROWS, D)
    routed = jnp.zeros((TOK2, D), jnp.float32)
    for top_step in range(TOP_K):
        picked = expert_out[buffer_row[:, top_step]].astype(jnp.float32)
        routed = routed + route_weights[:, top_step, None] * picked
    shared_gate_val = jnp.dot(normed, shared_gate, preferred_element_type=jnp.float32)
    shared_up_val = jnp.dot(normed, shared_up, preferred_element_type=jnp.float32)
    shared_hidden = (jax.nn.silu(shared_gate_val) * shared_up_val).astype(jnp.bfloat16)
    block_width = SHARED_DIM // N_TP
    shared_sum = jnp.zeros((TOK2, D), jnp.float32)
    for block_idx in range(N_TP):
        lower = block_idx * block_width
        partial_sum = jnp.dot(shared_hidden[:, lower:lower + block_width], shared_down[lower:lower + block_width], preferred_element_type=jnp.float32).astype(jnp.bfloat16)
        partial_sum = lax.optimization_barrier(partial_sum)
        shared_sum = shared_sum + partial_sum.astype(jnp.float32)
    return (routed + shared_sum).astype(jnp.bfloat16)

def reference(pool_input, pool_map, pool_scale, out_proj, moe_input, norm_gain, routes, route_weights, expert_gate, expert_up, expert_down, shared_gate, shared_up, shared_down):
    mixer_output = pool_mixer(pool_input, pool_map, pool_scale, out_proj)
    moe_output = moe_layer(moe_input, norm_gain, routes, route_weights, expert_gate, expert_up, expert_down, shared_gate, shared_up, shared_down)
    return (mixer_output, moe_output)
```

```python
import jax
import jax.numpy as jnp
from jax import lax
from jax.experimental import pallas as pl
from jax.experimental.pallas import tpu as pltpu
from jax.sharding import PartitionSpec as P

windows = (2, 4, 8, 16)
reach_back = 15
eps = 1e-05


def passed_along(block, axis, distance):
    devices = range(lax.axis_size(axis))
    route = [(i - distance, i) for i in devices if i - distance in devices]
    return lax.ppermute(block, axis, route)


def pool_branch(pool_input, pool_map, pool_scale, out_proj):
    row_count = pool_input.shape[0]
    channels = pool_input.shape[1]
    group_dim = pool_map.shape[1]
    local_groups = channels // group_dim
    tp_rank = lax.axis_index("tp")
    ep_rank = lax.axis_index("ep")
    earlier_rows = passed_along(pool_input[row_count - reach_back :], "ep", 1)
    values = pool_input.astype(jnp.float32)
    extended = jnp.concatenate([earlier_rows.astype(jnp.float32), values], axis=0)
    position = (ep_rank * row_count + jnp.arange(row_count, dtype=jnp.int32)).astype(jnp.float32)
    group_ids = tp_rank * local_groups + jnp.arange(channels, dtype=jnp.int32) // group_dim
    group_kind = group_ids % 4
    running = jnp.zeros((row_count, channels), jnp.float32)
    pooled = -values
    for lag_step in range(reach_back + 1):
        running = running + extended[reach_back - lag_step : reach_back - lag_step + row_count]
        if lag_step + 1 in windows:
            kind_id = windows.index(lag_step + 1)
            counts = jnp.minimum(position + 1.0, float(lag_step + 1))
            select = (group_kind == kind_id).astype(jnp.float32)
            pooled = pooled + select[None, :] * running / counts[:, None]
    pooled = pooled.astype(jnp.bfloat16)
    my_maps = lax.dynamic_slice_in_dim(pool_map, tp_rank * local_groups, local_groups, 0)
    my_scale = lax.dynamic_slice_in_dim(pool_scale, tp_rank * channels, channels, 0)
    mapped = jnp.einsum(
        "rgc,gcd->rgd",
        pooled.reshape(row_count, local_groups, group_dim),
        my_maps,
        preferred_element_type=jnp.float32,
    )
    group_out = (mapped.reshape(row_count, channels) * my_scale[None, :]).astype(jnp.bfloat16)
    return jnp.dot(group_out, out_proj, preferred_element_type=jnp.float32)


def dispatch_rows(routes, expert_count, capacity):
    tok_count, top_count = routes.shape
    flat_ids = routes.reshape(tok_count * top_count)
    one_hot = (flat_ids[:, None] == jnp.arange(expert_count, dtype=jnp.int32)[None, :]).astype(
        jnp.int32
    )
    earlier = jnp.cumsum(one_hot, axis=0) - one_hot
    slot_ids = jnp.sum(earlier * one_hot, axis=1)
    return (flat_ids * capacity + slot_ids).reshape(tok_count, top_count)


def per_device(
    pool_input,
    pool_map,
    pool_scale,
    out_proj,
    moe_input,
    norm_gain,
    routes,
    route_weights,
    expert_gate,
    expert_up,
    expert_down,
    shared_gate,
    shared_up,
    shared_down,
):
    mixer_part = pool_branch(pool_input, pool_map, pool_scale, out_proj)
    values = moe_input.astype(jnp.float32)
    centre = values - jnp.mean(values, axis=1, keepdims=True)
    variance = jnp.mean(centre * centre, axis=1, keepdims=True)
    normed = (centre * lax.rsqrt(variance + eps) * norm_gain[None, :]).astype(jnp.bfloat16)
    expert_count = lax.axis_size("ep")
    tok_count = moe_input.shape[0]
    top_count = routes.shape[1]
    capacity = (3 * tok_count * top_count + 2 * expert_count - 1) // (2 * expert_count)
    slot_index = dispatch_rows(routes, expert_count, capacity)
    buffer_len = expert_count * capacity
    targets = jnp.arange(buffer_len, dtype=jnp.int32)[:, None]
    placing = jnp.zeros((buffer_len, tok_count), jnp.float32)
    for top_step in range(top_count):
        placing = placing + (targets == slot_index[None, :, top_step]).astype(jnp.float32)
    outgoing = jnp.dot(
        placing.astype(jnp.bfloat16), normed, preferred_element_type=jnp.float32
    ).astype(jnp.bfloat16)
    gate_weight = expert_gate[0]
    up_weight = expert_up[0]
    down_weight = expert_down[0]
    tp_rank = lax.axis_index("tp")
    slice_width = outgoing.shape[1] // lax.axis_size("tp")
    my_slice = lax.dynamic_slice_in_dim(outgoing, tp_rank * slice_width, slice_width, 1)
    arrived = lax.all_to_all(my_slice, "ep", split_axis=0, concat_axis=0, tiled=True)
    shard_cols = lax.all_gather(arrived, "tp", axis=1, tiled=True)
    gate_val = jnp.dot(shard_cols, gate_weight, preferred_element_type=jnp.float32)
    up_val = jnp.dot(shard_cols, up_weight, preferred_element_type=jnp.float32)
    hidden = (jax.nn.silu(gate_val) * up_val).astype(jnp.bfloat16)
    expert_result = jnp.dot(
        lax.all_gather(hidden, "tp", axis=1, tiled=True),
        down_weight,
        preferred_element_type=jnp.float32,
    ).astype(jnp.bfloat16)
    returned = lax.all_to_all(expert_result, "ep", split_axis=0, concat_axis=0, tiled=True)
    routed = jnp.zeros((tok_count, returned.shape[1]), jnp.float32)
    for top_step in range(top_count):
        picked = returned[slot_index[:, top_step]].astype(jnp.float32)
        routed = routed + route_weights[:, top_step, None] * picked
    shared_gate_val = jnp.dot(normed, shared_gate, preferred_element_type=jnp.float32)
    shared_up_val = jnp.dot(normed, shared_up, preferred_element_type=jnp.float32)
    shared_hidden = (jax.nn.silu(shared_gate_val) * shared_up_val).astype(jnp.bfloat16)
    shared_part = jnp.dot(shared_hidden, shared_down, preferred_element_type=jnp.float32)
    mixer_sum, shared_sum = (
        lax.psum_scatter(
            mixer_part.astype(jnp.bfloat16), "tp", scatter_dimension=1, tiled=True
        ).astype(jnp.float32),
        lax.psum_scatter(
            shared_part.astype(jnp.bfloat16), "tp", scatter_dimension=1, tiled=True
        ).astype(jnp.float32),
    )
    return (mixer_sum.astype(jnp.bfloat16), (routed + shared_sum).astype(jnp.bfloat16))


HALO = 16
Z_SIDE, X_SIDE, Y_SIDE, CORES = 4, 2, 2, 2
MIX_PARTS = 4


def fused_kernel(
    pool_h, map_h, scale_h, proj_h, moe_h, gain_h, route_h, rw_h, gate_h, up_h, down_h, sg_h, su_h, sd_h,
    mix_out, moe_out,
    pool_v, map_v, scale_v, proj_v, moe_v, gain_v, route_v, rw_v, gate_v, up_v, down_v, sg_v, su_v, sd_v,
    halo_v, ext_v, group_v, mix_v, mix_core, mix_y, mix_send,
    raw_v, comp_v, xs_v, wts_v, slot_v, pick_v, mixw_v, hid_v, outx_v, pair_v, acc_v, part_z, part_send,
    sh_v, sh_core, sh_y, sh_send,
    load_sem, halo_sem, z_send, z_recv, x_send, x_recv, y_send, y_recv, c_send, c_recv,
    w_send, w_recv, h_send, h_recv, rx_send, rx_recv, rz_send, rz_recv, m_send, m_recv, ms_send, ms_recv,
):
    f32, bf16 = jnp.float32, jnp.bfloat16
    e = lax.axis_index("ep")
    t = lax.axis_index("tp")
    n_ep = Z_SIDE * X_SIDE
    z, x = e // X_SIDE, e % X_SIDE
    y, c = t // CORES, t % CORES
    toks = moe_h.shape[0]
    width = moe_h.shape[1]
    cap = comp_v.shape[0] // n_ep
    part = width // (Y_SIDE * CORES)
    hid = gate_h.shape[2]
    near = NEAR * part // 8
    rest = part - near
    inner = (z > 0) & (z < Z_SIDE - 1)
    kin = [z, z + 1 - 2 * (z % 2), (z + 2) % 4, 3 - z]
    turn = [0, jnp.where(inner, 3, 1), 2, jnp.where(inner, 1, 3)]
    zs = [z, jnp.where(inner, kin[3], kin[1]), kin[2], jnp.where(inner, kin[1], kin[3])]
    xs = [x, 1 - x]
    ex = z * X_SIDE + xs[1]
    ty, tc, tyc = (1 - y) * CORES + c, y * CORES + 1 - c, (1 - y) * CORES + 1 - c

    barrier = pltpu.get_barrier_semaphore()
    for k in range(Z_SIDE):
        for j in range(X_SIDE):
            if k or j:
                pl.semaphore_signal(barrier, inc=1, device_id={"ep": zs[k] * X_SIDE + xs[j], "tp": t},
                                    device_id_type=pl.DeviceIdType.MESH)
    for peer in (ty, tc):
        pl.semaphore_signal(barrier, inc=1, device_id={"ep": e, "tp": peer},
                            device_id_type=pl.DeviceIdType.MESH)

    def raw_row(k):
        return pl.multiple_of(zs[k] * toks, toks)

    def row0(k, j):
        return pl.multiple_of((zs[k] * X_SIDE + xs[j]) * cap, cap)

    def pair_row(k):
        return pl.multiple_of(zs[k] * X_SIDE * cap, X_SIDE * cap)

    def col(s, shift=0):
        return pl.multiple_of(s * part + shift, 128)

    loads = {}
    for i, (name, src, dst) in enumerate((
        ("moe", moe_h, moe_v), ("gain", gain_h, gain_v),
        ("route", route_h, route_v), ("rw", rw_h, rw_v), ("pool", pool_h, pool_v),
        ("map", map_h.at[pl.ds(t * map_v.shape[0], map_v.shape[0])], map_v),
        ("scale", scale_h.at[:, pl.ds(pl.multiple_of(t * scale_v.shape[1], 128), scale_v.shape[1])], scale_v),
        ("sg", sg_h, sg_v), ("su", su_h, su_v), ("sd", sd_h, sd_v), ("proj", proj_h, proj_v),
        ("gate", gate_h.at[0], gate_v), ("up", up_h.at[0], up_v), ("down", down_h.at[0], down_v),
    )):
        cp = pltpu.make_async_copy(src, dst, load_sem.at[i])
        cp.start()
        loads[name] = cp

    sent = []

    def remote(src, dst, ssem, rsem, ep, tp):
        return pltpu.make_async_remote_copy(src_ref=src, dst_ref=dst, send_sem=ssem, recv_sem=rsem,
                                            device_id={"ep": ep, "tp": tp},
                                            device_id_type=pl.DeviceIdType.MESH)

    def start(cp):
        cp.start()
        sent.append(cp)

    def push(src, dst, ssem, rsem, ep, tp):
        start(remote(src, dst, ssem, rsem, ep, tp))

    def arrived(ref, ssem, rsem):
        pltpu.make_async_remote_copy(src_ref=ref, dst_ref=ref, send_sem=ssem, recv_sem=rsem,
                                     device_id={"ep": e, "tp": tc},
                                     device_id_type=pl.DeviceIdType.MESH).wait_recv()

    def routing(k):
        w = wts_v[k]
        a = lax.broadcasted_iota(jnp.int32, (toks, toks), 0)
        b = lax.broadcasted_iota(jnp.int32, (toks, toks), 1)
        before = jnp.where(a < b, 1.0, 0.0).astype(bf16)
        slot = jnp.dot(jnp.where(w > 0.0, 1.0, 0.0).astype(bf16), before, preferred_element_type=f32)
        slot_v[k] = jnp.where(w > 0.0, slot, -1024.0)
        own_row, other_row = slot_v[k, pl.ds(e, 1), :], slot_v[k, pl.ds(ex, 1), :]
        r = lax.broadcasted_iota(jnp.int32, (X_SIDE * cap, toks), 0).astype(f32)
        place = jnp.where(r < float(cap), jnp.broadcast_to(own_row, r.shape),
                          jnp.broadcast_to(other_row, r.shape) + float(cap))
        pick_v[k] = jnp.where(place == r, 1.0, 0.0).astype(bf16)

        def turned(row):
            return jnp.sum(jnp.where(a == b, jnp.broadcast_to(row, (toks, toks)), 0.0), axis=1, keepdims=True)

        s = lax.broadcasted_iota(jnp.int32, (toks, X_SIDE * cap), 1).astype(f32)
        first = s < float(cap)
        place = jnp.where(first, turned(own_row), turned(other_row) + float(cap))
        value = jnp.where(first, turned(wts_v[k, pl.ds(e, 1), :]), turned(wts_v[k, pl.ds(ex, 1), :]))
        mixw_v[k] = jnp.where(place == s, value, 0.0).astype(bf16)

    loads["moe"].wait()
    loads["gain"].wait()
    own = raw_row(0)

    def norm_step(i, carry):
        r = pl.multiple_of(i * 16, 16)
        v = moe_v[pl.ds(r, 16), :].astype(f32)
        cen = v - jnp.mean(v, axis=1, keepdims=True)
        var = jnp.mean(cen * cen, axis=1, keepdims=True)
        raw_v[pl.ds(own + r, 16), :] = (cen * lax.rsqrt(var + eps) * gain_v[...]).astype(bf16)
        return carry

    lax.fori_loop(0, toks // 16, norm_step, 0, unroll=2)
    loads["pool"].wait()
    loads["route"].wait()
    loads["rw"].wait()
    ids = lax.broadcasted_iota(jnp.int32, (n_ep, toks), 0)
    weights = jnp.zeros((n_ep, toks), f32)
    for top_step in range(route_v.shape[0]):
        named = jnp.broadcast_to(route_v[top_step:top_step + 1, :], (n_ep, toks)) == ids
        weights = weights + jnp.where(named, jnp.broadcast_to(rw_v[top_step:top_step + 1, :], (n_ep, toks)), 0.0)
    wts_v[0] = weights

    pl.semaphore_wait(barrier, n_ep - 1 + 2)

    for k in range(1, Z_SIDE):
        push(wts_v.at[0], wts_v.at[k], w_send.at[k], w_recv.at[k], kin[k] * X_SIDE + x, t)

    count = pool_v.shape[0]
    tail_ref = pool_v.at[pl.ds(count - HALO, HALO), :]

    def halo_copy(target):
        return pltpu.make_async_remote_copy(src_ref=tail_ref, dst_ref=halo_v, send_sem=halo_sem.at[0],
                                            recv_sem=halo_sem.at[1], device_id={"ep": target, "tp": t},
                                            device_id_type=pl.DeviceIdType.MESH)

    @pl.when(e < n_ep - 1)
    def _():
        halo_copy(e + 1).start()

    def spans():
        return ((col(t), part), (col(ty, near), rest))

    def raw_ref(k, i):
        c0, n = spans()[i]
        return raw_v.at[pl.ds(pl.multiple_of(kin[k] * toks, toks), toks), pl.ds(c0, n)]

    handed = []

    def hop(k, to, at, slot, i):
        return pltpu.make_async_remote_copy(
            src_ref=raw_ref(k, i), dst_ref=raw_ref(k, i), send_sem=z_send.at[slot, i], recv_sem=z_recv.at[at, i],
            device_id={"ep": kin[to] * X_SIDE + x, "tp": t}, device_id_type=pl.DeviceIdType.MESH)

    def hand(k, to, at, slot, i):
        handed.append((k, to, at, slot, i))
        hop(k, to, at, slot, i).start()

    for i in (0, 1):
        cp = hop(0, 1, 1, 0, i)
        cp.start()
        sent.append(cp)

        @pl.when(inner)
        def _():
            hand(0, 3, 3, 1, i)

    step = 256

    def gather(k, i):
        c0, n = spans()[i]
        for q in range(n // step):
            cq = pl.ds(pl.multiple_of(c0 + q * step, 128), step)
            o = jnp.dot(pick_v[turn[k]], raw_v[pl.ds(raw_row(k), toks), cq], preferred_element_type=f32).astype(bf16)
            comp_v[pl.ds(row0(k, 0), cap), cq] = o[:cap]
            xs_v[k * cap:(k + 1) * cap, cq] = o[cap:]

    def x_copy(k, i):
        c0, n = spans()[i]
        return remote(xs_v.at[k * cap:(k + 1) * cap, pl.ds(c0, n)], comp_v.at[pl.ds(row0(k, 0), cap), pl.ds(c0, n)],
                      x_send.at[k, i], x_recv.at[k, i], ex, t)

    def x_push(k, i):
        start(x_copy(k, i))

    def near_ref(k, j, s):
        return comp_v.at[pl.ds(row0(k, j), cap), pl.ds(col(s), near)]

    def near_copy(k, j):
        return remote(near_ref(k, j, t), near_ref(k, j, t), y_send.at[k, j], y_recv.at[k, j], e, ty)

    def near_push(k, j):
        start(near_copy(k, j))

    routing(0)
    for i in (0, 1):
        gather(0, i)
        x_push(0, i)

    def gather_rest(c0, n):
        for q in range(n // step):
            cq = pl.ds(pl.multiple_of(c0 + q * step, 128), step)
            comp_v[pl.ds(row0(0, 0), cap), cq] = jnp.dot(
                pick_v[0, :cap], raw_v[pl.ds(own, toks), cq], preferred_element_type=f32).astype(bf16)

    gather_rest(col(ty), near)
    gather_rest(col(tc), part)
    gather_rest(col(tyc), part)

    def z_wait(k, i):
        arrived(raw_ref(k, i), z_send.at[k, i], z_recv.at[k, i])

    def w_arrive(k):
        arrived(wts_v.at[k], w_send.at[k], w_recv.at[k])
        routing(k)

    def rows_out(k, i):
        go = start if k < 3 else lambda cp: cp.start()
        gather(k, i)
        go(x_copy(k, i))
        if i == 0:
            go(near_copy(k, 0))

    def z_piece(k, i):
        if k < 3:
            z_wait(k, i)

            @pl.when(inner)
            def _():
                if k == 1:
                    hand(1, 3, 2, 2, i)
                    z_wait(3, i)
                    hand(3, 1, 2, 3, i)
                else:
                    hand(2, 1, 3, 4, i)

            rows_out(k, i)
        else:
            z_wait(3, i)
            rows_out(k, i)

    def early():
        @pl.when(inner)
        def _():
            for i in (0, 1):
                rows_out(3, i)

    def late(i):
        @pl.when(jnp.logical_not(inner))
        def _():
            z_piece(3, i)

    def x_piece(k, i):
        c0, n = spans()[i]
        arrived(comp_v.at[pl.ds(row0(k, 1), cap), pl.ds(c0, n)], x_send.at[k, i], x_recv.at[k, i])
        if i == 0:
            near_push(k, 1)

    def pair_ref(k, s):
        if k == 0:
            return comp_v.at[pl.ds(row0(0, 1), cap), pl.ds(col(s), part)]
        return comp_v.at[pl.ds(pair_row(k), X_SIDE * cap), pl.ds(col(s), part)]

    def y_arrive(k):
        for j in (0, 1):
            if k or j:
                arrived(near_ref(k, j, ty), y_send.at[k, j], y_recv.at[k, j])
        for i, s in enumerate((t, ty)):
            push(pair_ref(k, s), pair_ref(k, s), c_send.at[k, i], c_recv.at[k, i], e, tc)

    def core_arrive(k):
        for i, s in enumerate((tc, tyc)):
            arrived(pair_ref(k, s), c_send.at[k, i], c_recv.at[k, i])

    def hid_ref(k, s):
        return hid_v.at[pl.ds(pair_row(k), X_SIDE * cap), pl.ds(pl.multiple_of(s * hid, 128), hid)]

    def expert_in(k):
        rows = comp_v[pl.ds(pair_row(k), X_SIDE * cap), :]
        g = jnp.dot(rows, gate_v[...], preferred_element_type=f32)
        u = jnp.dot(rows, up_v[...], preferred_element_type=f32)
        hid_ref(k, t)[...] = (g / (1.0 + jnp.exp(-g)) * u).astype(bf16)
        push(hid_ref(k, t), hid_ref(k, t), h_send.at[k, 0], h_recv.at[k, 0], e, ty)
        push(hid_ref(k, t), hid_ref(k, t), h_send.at[k, 1], h_recv.at[k, 1], e, tc)

    def hid_forward(k):
        arrived(hid_ref(k, ty), h_send.at[k, 0], h_recv.at[k, 0])
        push(hid_ref(k, ty), hid_ref(k, ty), h_send.at[k, 2], h_recv.at[k, 2], e, tc)

    half = part // 2

    def half_push(k, h):
        cols = pl.ds(h * half, half)
        push(outx_v.at[k, :, cols], pair_v.at[k, pl.ds(cap, cap), cols], rx_send.at[k, h],
             rx_recv.at[k, h], ex, t)

    def out_push(k):
        half_push(k, 0)
        half_push(k, 1)

    def expert_out(k, send=True):
        arrived(hid_ref(k, tc), h_send.at[k, 1], h_recv.at[k, 1])
        arrived(hid_ref(k, tyc), h_send.at[k, 2], h_recv.at[k, 2])
        for j in (1, 0):
            rows = hid_v[pl.ds(row0(k, j), cap), :]
            for q in range(part // 256):
                o = jnp.dot(rows, down_v[:, q * 256:(q + 1) * 256], preferred_element_type=f32).astype(bf16)
                if j:
                    outx_v[k, :, q * 256:(q + 1) * 256] = o
                    if send and (q + 1) * 256 % half == 0:
                        half_push(k, (q + 1) * 256 // half - 1)
                else:
                    pair_v[k, :cap, q * 256:(q + 1) * 256] = o

    def sum_x(k):
        for h in (0, 1):
            cols = pl.ds(h * half, half)
            arrived(pair_v.at[k, pl.ds(cap, cap), cols], rx_send.at[k, h], rx_recv.at[k, h])
            both = jnp.dot(mixw_v[turn[k]], pair_v[k, :, cols], preferred_element_type=f32)
            if k:
                part_send[k, :, cols] = both.astype(bf16)
                push(part_send.at[k, :, cols], part_z.at[turn[k], :, cols], rz_send.at[k, h],
                     rz_recv.at[turn[k], h], zs[k] * X_SIDE + x, t)
            else:
                acc_v[:, cols] = both

    def shared():
        loads["sg"].wait()
        loads["su"].wait()
        rows = raw_v[pl.ds(own, toks), :]
        g = jnp.dot(rows, sg_v[...], preferred_element_type=f32)
        u = jnp.dot(rows, su_v[...], preferred_element_type=f32)
        shared_hidden = (g / (1.0 + jnp.exp(-g)) * u).astype(bf16)
        loads["sd"].wait()
        for q in range(width // 512):
            sh_v[:, q * 512:(q + 1) * 512] = jnp.dot(
                shared_hidden, sd_v[:, q * 512:(q + 1) * 512], preferred_element_type=f32).astype(bf16)
        for i, s in enumerate((tc, tyc)):
            push(sh_v.at[:, pl.ds(col(s), part)], sh_core.at[i], m_send.at[0, i], m_recv.at[0, i], e, tc)

    def pool():
        @pl.when(e == 0)
        def _():
            halo_v[...] = jnp.zeros_like(halo_v)

        @pl.when(e > 0)
        def _():
            halo_copy(e - 1).wait_recv()

        ext_v[:HALO, :] = halo_v[...].astype(f32)
        ext_v[HALO:, :] = pool_v[...].astype(f32)
        loads["map"].wait()
        loads["scale"].wait()
        dim = map_v.shape[1]
        position = (e * count + lax.broadcasted_iota(jnp.int32, (count, dim), 0)).astype(f32)
        for grp in range(map_v.shape[0]):
            w = windows[grp % 4]
            cs = slice(grp * dim, (grp + 1) * dim)
            values = ext_v[HALO:, cs]
            running = values
            for lag in range(1, w):
                running = running + ext_v[HALO - lag:HALO - lag + count, cs]
            pooled = (running / jnp.minimum(position + 1.0, float(w)) - values).astype(bf16)
            mapped = jnp.dot(pooled, map_v[grp], preferred_element_type=f32)
            group_v[:, cs] = (mapped * scale_v[:, cs]).astype(bf16)

    def proj():
        loads["proj"].wait()

        def proj_step(q, carry):
            cq = pl.ds(pl.multiple_of(q * 512, 512), 512)
            mix_v[:, cq] = jnp.dot(group_v[...], proj_v[:, cq], preferred_element_type=f32).astype(bf16)
            return carry

        lax.fori_loop(0, width // 512, proj_step, 0)
        for i, s in enumerate((tc, tyc)):
            push(mix_v.at[:, pl.ds(col(s), part)], mix_core.at[i], m_send.at[1, i], m_recv.at[1, i], e, tc)

    def core_sum(which, own_ref, core_ref, send_ref):
        for i in (0, 1):
            arrived(core_ref.at[i], m_send.at[which, i], m_recv.at[which, i])
        send_ref[...] = (own_ref[:, pl.ds(col(ty), part)].astype(f32) + core_ref[1].astype(f32)).astype(bf16)

    def sh_core_sum():
        core_sum(0, sh_v, sh_core, sh_send)

    def sh_push():
        push(sh_send, sh_y, m_send.at[0, 2], m_recv.at[0, 2], e, ty)

    def mix_core_sum():
        core_sum(1, mix_v, mix_core, mix_send)

    piece = count // MIX_PARTS

    def mix_push(n):
        push(mix_send.at[pl.ds(n * piece, piece)], mix_y.at[pl.ds(n * piece, piece)], ms_send.at[n], ms_recv.at[n],
             e, ty)

    def mix_final():
        for n in range(MIX_PARTS):
            arrived(mix_y.at[pl.ds(n * piece, piece)], ms_send.at[n], ms_recv.at[n])
        mix_out[...] = (mix_v[:, pl.ds(col(t), part)].astype(f32) + mix_core[0].astype(f32)
                        + mix_y[...].astype(f32)).astype(bf16)

    def sh_final():
        arrived(sh_y, m_send.at[0, 2], m_recv.at[0, 2])
        acc_v[...] = (acc_v[...] + sh_v[:, pl.ds(col(t), part)].astype(f32) + sh_core[0].astype(f32)
                      + sh_y[...].astype(f32))

    def z_final(h):
        cols = pl.ds(h * half, half)
        total = acc_v[:, cols]
        for k in (1, 2, 3):
            arrived(part_z.at[k, :, cols], rz_send.at[k, h], rz_recv.at[k, h])
            total = total + part_z[k, :, cols].astype(f32)
        moe_out[:, cols] = total.astype(bf16)

    def experts_loaded():
        loads["gate"].wait()
        loads["up"].wait()

    shared()
    w_arrive(1)
    w_arrive(2)
    w_arrive(3)
    pool()
    sh_core_sum()
    proj()
    x_piece(0, 0)
    mix_core_sum()
    z_piece(1, 0)
    x_piece(0, 1)
    z_piece(1, 1)
    y_arrive(0)
    x_piece(1, 0)
    core_arrive(0)
    experts_loaded()
    expert_in(0)
    z_piece(2, 0)
    x_piece(1, 1)
    y_arrive(1)
    core_arrive(1)
    expert_in(1)
    z_piece(2, 1)
    early()
    hid_forward(0)
    x_piece(2, 0)
    loads["down"].wait()
    expert_out(0, False)
    hid_forward(1)
    x_piece(2, 1)
    y_arrive(2)
    late(0)
    expert_out(1, False)
    core_arrive(2)
    expert_in(2)
    late(1)
    out_push(1)
    x_piece(3, 0)
    hid_forward(2)
    x_piece(3, 1)
    y_arrive(3)
    expert_out(2)
    core_arrive(3)
    expert_in(3)
    sh_push()
    mix_push(0)
    mix_push(1)
    mix_push(2)
    mix_push(3)
    sum_x(1)
    hid_forward(3)
    sum_x(2)
    expert_out(3)
    out_push(0)
    sum_x(3)
    sum_x(0)
    sh_final()
    mix_final()
    z_final(0)
    z_final(1)

    for cp in sent:
        cp.wait_send()
    for i in (0, 1):
        x_copy(3, i).wait_send()
    near_copy(3, 0).wait_send()

    @pl.when(inner)
    def _():
        for which in handed:
            hop(*which).wait_send()

    @pl.when(e < n_ep - 1)
    def _():
        halo_copy(e + 1).wait_send()


NEAR = 2


def per_device_fused(
    pool_input, pool_map, pool_scale, out_proj, moe_input, norm_gain, routes, route_weights,
    expert_gate, expert_up, expert_down, shared_gate, shared_up, shared_down,
):
    f32, bf16 = jnp.float32, jnp.bfloat16
    n_ep = lax.axis_size("ep")
    toks, width = moe_input.shape
    top_count = routes.shape[1]
    count, channels = pool_input.shape
    dim = pool_map.shape[1]
    part = width // lax.axis_size("tp")
    cap = (3 * toks * top_count + 2 * n_ep - 1) // (2 * n_ep)
    dma = pltpu.SemaphoreType.DMA
    return pl.pallas_call(
        fused_kernel,
        out_shape=(jax.ShapeDtypeStruct((count, part), bf16), jax.ShapeDtypeStruct((toks, part), bf16)),
        in_specs=[pl.BlockSpec(memory_space=pl.ANY)] * 14,
        out_specs=(pl.BlockSpec(memory_space=pltpu.VMEM), pl.BlockSpec(memory_space=pltpu.VMEM)),
        scratch_shapes=[
            pltpu.VMEM((count, channels), bf16),
            pltpu.VMEM((channels // dim, dim, dim), bf16),
            pltpu.VMEM((1, channels), f32),
            pltpu.VMEM(out_proj.shape, bf16),
            pltpu.VMEM((toks, width), bf16),
            pltpu.VMEM((1, width), f32),
            pltpu.VMEM((top_count, toks), jnp.int32),
            pltpu.VMEM((top_count, toks), f32),
            pltpu.VMEM(expert_gate.shape[1:], bf16),
            pltpu.VMEM(expert_up.shape[1:], bf16),
            pltpu.VMEM(expert_down.shape[1:], bf16),
            pltpu.VMEM(shared_gate.shape, bf16),
            pltpu.VMEM(shared_up.shape, bf16),
            pltpu.VMEM(shared_down.shape, bf16),
            pltpu.VMEM((HALO, channels), bf16),
            pltpu.VMEM((HALO + count, channels), f32),
            pltpu.VMEM((count, channels), bf16),
            pltpu.VMEM((count, width), bf16),
            pltpu.VMEM((2, count, part), bf16),
            pltpu.VMEM((count, part), bf16),
            pltpu.VMEM((count, part), bf16),
            pltpu.VMEM((Z_SIDE * toks, width), bf16),
            pltpu.VMEM((n_ep * cap, width), bf16),
            pltpu.VMEM((Z_SIDE * cap, width), bf16),
            pltpu.VMEM((Z_SIDE, n_ep, toks), f32),
            pltpu.VMEM((Z_SIDE, n_ep, toks), f32),
            pltpu.VMEM((Z_SIDE, X_SIDE * cap, toks), bf16),
            pltpu.VMEM((Z_SIDE, toks, X_SIDE * cap), bf16),
            pltpu.VMEM((n_ep * cap, expert_down.shape[1]), bf16),
            pltpu.VMEM((Z_SIDE, cap, part), bf16),
            pltpu.VMEM((Z_SIDE, X_SIDE * cap, part), bf16),
            pltpu.VMEM((toks, part), f32),
            pltpu.VMEM((Z_SIDE, toks, part), bf16),
            pltpu.VMEM((Z_SIDE, toks, part), bf16),
            pltpu.VMEM((toks, width), bf16),
            pltpu.VMEM((2, toks, part), bf16),
            pltpu.VMEM((toks, part), bf16),
            pltpu.VMEM((toks, part), bf16),
            dma((14,)), dma((2,)),
            dma((5, 2)), dma((4, 2)), dma((4, 2)), dma((4, 2)), dma((4, 2)), dma((4, 2)),
            dma((4, 2)), dma((4, 2)), dma((4,)), dma((4,)), dma((4, 3)), dma((4, 3)),
            dma((4, 2)), dma((4, 2)), dma((4, 2)), dma((4, 2)), dma((2, 3)), dma((2, 3)),
            dma((MIX_PARTS,)), dma((MIX_PARTS,)),
        ],
        compiler_params=pltpu.CompilerParams(
            collective_id=0, has_side_effects=True, vmem_limit_bytes=60 * 1024 * 1024),
    )(
        pool_input, pool_map, pool_scale.reshape(1, -1), out_proj, moe_input, norm_gain.reshape(1, -1),
        routes.T, route_weights.T, expert_gate, expert_up, expert_down, shared_gate, shared_up, shared_down,
    )


def solution(mesh):
    plane = mesh.shape["ep"] == Z_SIDE * X_SIDE and mesh.shape["tp"] == Y_SIDE * CORES
    body = per_device_fused if plane else per_device
    return jax.shard_map(
        body,
        mesh=mesh,
        in_specs=(
            P("ep", "tp"),
            P(),
            P(),
            P("tp", None),
            P("ep", None),
            P(),
            P("ep", None),
            P("ep", None),
            P("ep", None, "tp"),
            P("ep", None, "tp"),
            P("ep", None, "tp"),
            P(None, "tp"),
            P(None, "tp"),
            P("tp", None),
        ),
        out_specs=(P("ep", "tp"), P("ep", "tp")),
        check_vma=False,
    )
```

```python
import jax
import jax.numpy as jnp
from jax import lax
from jax.experimental import pallas as pl
from jax.experimental.pallas import tpu as pltpu
from jax.sharding import PartitionSpec as P

windows = (2, 4, 8, 16)
reach_back = 15
eps = 1e-05


def passed_along(block, axis, distance):
    devices = range(lax.axis_size(axis))
    route = [(i - distance, i) for i in devices if i - distance in devices]
    return lax.ppermute(block, axis, route)


def pool_branch(pool_input, pool_map, pool_scale, out_proj):
    row_count = pool_input.shape[0]
    channels = pool_input.shape[1]
    group_dim = pool_map.shape[1]
    local_groups = channels // group_dim
    tp_rank = lax.axis_index("tp")
    ep_rank = lax.axis_index("ep")
    earlier_rows = passed_along(pool_input[row_count - reach_back :], "ep", 1)
    values = pool_input.astype(jnp.float32)
    extended = jnp.concatenate([earlier_rows.astype(jnp.float32), values], axis=0)
    position = (ep_rank * row_count + jnp.arange(row_count, dtype=jnp.int32)).astype(jnp.float32)
    group_ids = tp_rank * local_groups + jnp.arange(channels, dtype=jnp.int32) // group_dim
    group_kind = group_ids % 4
    running = jnp.zeros((row_count, channels), jnp.float32)
    pooled = -values
    for lag_step in range(reach_back + 1):
        running = running + extended[reach_back - lag_step : reach_back - lag_step + row_count]
        if lag_step + 1 in windows:
            kind_id = windows.index(lag_step + 1)
            counts = jnp.minimum(position + 1.0, float(lag_step + 1))
            select = (group_kind == kind_id).astype(jnp.float32)
            pooled = pooled + select[None, :] * running / counts[:, None]
    pooled = pooled.astype(jnp.bfloat16)
    my_maps = lax.dynamic_slice_in_dim(pool_map, tp_rank * local_groups, local_groups, 0)
    my_scale = lax.dynamic_slice_in_dim(pool_scale, tp_rank * channels, channels, 0)
    mapped = jnp.einsum(
        "rgc,gcd->rgd",
        pooled.reshape(row_count, local_groups, group_dim),
        my_maps,
        preferred_element_type=jnp.float32,
    )
    group_out = (mapped.reshape(row_count, channels) * my_scale[None, :]).astype(jnp.bfloat16)
    return jnp.dot(group_out, out_proj, preferred_element_type=jnp.float32)


def dispatch_rows(routes, expert_count, capacity):
    tok_count, top_count = routes.shape
    flat_ids = routes.reshape(tok_count * top_count)
    one_hot = (flat_ids[:, None] == jnp.arange(expert_count, dtype=jnp.int32)[None, :]).astype(
        jnp.int32
    )
    earlier = jnp.cumsum(one_hot, axis=0) - one_hot
    slot_ids = jnp.sum(earlier * one_hot, axis=1)
    return (flat_ids * capacity + slot_ids).reshape(tok_count, top_count)


def per_device(
    pool_input,
    pool_map,
    pool_scale,
    out_proj,
    moe_input,
    norm_gain,
    routes,
    route_weights,
    expert_gate,
    expert_up,
    expert_down,
    shared_gate,
    shared_up,
    shared_down,
):
    mixer_part = pool_branch(pool_input, pool_map, pool_scale, out_proj)
    values = moe_input.astype(jnp.float32)
    centre = values - jnp.mean(values, axis=1, keepdims=True)
    variance = jnp.mean(centre * centre, axis=1, keepdims=True)
    normed = (centre * lax.rsqrt(variance + eps) * norm_gain[None, :]).astype(jnp.bfloat16)
    expert_count = lax.axis_size("ep")
    tok_count = moe_input.shape[0]
    top_count = routes.shape[1]
    capacity = (3 * tok_count * top_count + 2 * expert_count - 1) // (2 * expert_count)
    slot_index = dispatch_rows(routes, expert_count, capacity)
    buffer_len = expert_count * capacity
    targets = jnp.arange(buffer_len, dtype=jnp.int32)[:, None]
    placing = jnp.zeros((buffer_len, tok_count), jnp.float32)
    for top_step in range(top_count):
        placing = placing + (targets == slot_index[None, :, top_step]).astype(jnp.float32)
    outgoing = jnp.dot(
        placing.astype(jnp.bfloat16), normed, preferred_element_type=jnp.float32
    ).astype(jnp.bfloat16)
    gate_weight = expert_gate[0]
    up_weight = expert_up[0]
    down_weight = expert_down[0]
    tp_rank = lax.axis_index("tp")
    slice_width = outgoing.shape[1] // lax.axis_size("tp")
    my_slice = lax.dynamic_slice_in_dim(outgoing, tp_rank * slice_width, slice_width, 1)
    arrived = lax.all_to_all(my_slice, "ep", split_axis=0, concat_axis=0, tiled=True)
    shard_cols = lax.all_gather(arrived, "tp", axis=1, tiled=True)
    gate_val = jnp.dot(shard_cols, gate_weight, preferred_element_type=jnp.float32)
    up_val = jnp.dot(shard_cols, up_weight, preferred_element_type=jnp.float32)
    hidden = (jax.nn.silu(gate_val) * up_val).astype(jnp.bfloat16)
    expert_result = jnp.dot(
        lax.all_gather(hidden, "tp", axis=1, tiled=True),
        down_weight,
        preferred_element_type=jnp.float32,
    ).astype(jnp.bfloat16)
    returned = lax.all_to_all(expert_result, "ep", split_axis=0, concat_axis=0, tiled=True)
    routed = jnp.zeros((tok_count, returned.shape[1]), jnp.float32)
    for top_step in range(top_count):
        picked = returned[slot_index[:, top_step]].astype(jnp.float32)
        routed = routed + route_weights[:, top_step, None] * picked
    shared_gate_val = jnp.dot(normed, shared_gate, preferred_element_type=jnp.float32)
    shared_up_val = jnp.dot(normed, shared_up, preferred_element_type=jnp.float32)
    shared_hidden = (jax.nn.silu(shared_gate_val) * shared_up_val).astype(jnp.bfloat16)
    shared_part = jnp.dot(shared_hidden, shared_down, preferred_element_type=jnp.float32)
    mixer_sum, shared_sum = (
        lax.psum_scatter(
            mixer_part.astype(jnp.bfloat16), "tp", scatter_dimension=1, tiled=True
        ).astype(jnp.float32),
        lax.psum_scatter(
            shared_part.astype(jnp.bfloat16), "tp", scatter_dimension=1, tiled=True
        ).astype(jnp.float32),
    )
    return (mixer_sum.astype(jnp.bfloat16), (routed + shared_sum).astype(jnp.bfloat16))


HALO = 16
Z_SIDE, X_SIDE, Y_SIDE, CORES = 4, 2, 2, 2
MIX_PARTS = 4


def fused_kernel(
    pool_h, map_h, scale_h, proj_h, moe_h, gain_h, route_h, rw_h, gate_h, up_h, down_h, sg_h, su_h, sd_h,
    mix_out, moe_out,
    pool_v, map_v, scale_v, proj_v, moe_v, gain_v, route_v, rw_v, gate_v, up_v, down_v, sg_v, su_v, sd_v,
    halo_v, ext_v, group_v, mix_v, mix_core, mix_y, mix_send,
    raw_v, comp_v, xs_v, wts_v, slot_v, pick_v, mixw_v, hid_v, outx_v, pair_v, acc_v, part_z, part_send,
    sh_v, sh_core, sh_y, sh_send,
    load_sem, halo_sem, z_send, z_recv, x_send, x_recv, y_send, y_recv, c_send, c_recv,
    w_send, w_recv, h_send, h_recv, rx_send, rx_recv, rz_send, rz_recv, m_send, m_recv, ms_send, ms_recv,
):
    f32, bf16 = jnp.float32, jnp.bfloat16
    e = lax.axis_index("ep")
    t = lax.axis_index("tp")
    n_ep = Z_SIDE * X_SIDE
    z, x = e // X_SIDE, e % X_SIDE
    y, c = t // CORES, t % CORES
    toks = moe_h.shape[0]
    width = moe_h.shape[1]
    cap = comp_v.shape[0] // n_ep
    part = width // (Y_SIDE * CORES)
    hid = gate_h.shape[2]
    near = NEAR * part // 8
    rest = part - near
    inner = (z > 0) & (z < Z_SIDE - 1)
    kin = [z, z + 1 - 2 * (z % 2), (z + 2) % 4, 3 - z]
    turn = [0, jnp.where(inner, 3, 1), 2, jnp.where(inner, 1, 3)]
    zs = [z, jnp.where(inner, kin[3], kin[1]), kin[2], jnp.where(inner, kin[1], kin[3])]
    xs = [x, 1 - x]
    ex = z * X_SIDE + xs[1]
    ty, tc, tyc = (1 - y) * CORES + c, y * CORES + 1 - c, (1 - y) * CORES + 1 - c

    barrier = pltpu.get_barrier_semaphore()
    for k in range(Z_SIDE):
        for j in range(X_SIDE):
            if k or j:
                pl.semaphore_signal(barrier, inc=1, device_id={"ep": zs[k] * X_SIDE + xs[j], "tp": t},
                                    device_id_type=pl.DeviceIdType.MESH)
    for peer in (ty, tc):
        pl.semaphore_signal(barrier, inc=1, device_id={"ep": e, "tp": peer},
                            device_id_type=pl.DeviceIdType.MESH)

    def raw_row(k):
        return pl.multiple_of(zs[k] * toks, toks)

    def row0(k, j):
        return pl.multiple_of((zs[k] * X_SIDE + xs[j]) * cap, cap)

    def pair_row(k):
        return pl.multiple_of(zs[k] * X_SIDE * cap, X_SIDE * cap)

    def col(s, shift=0):
        return pl.multiple_of(s * part + shift, 128)

    loads = {}
    for i, (name, src, dst) in enumerate((
        ("moe", moe_h, moe_v), ("gain", gain_h, gain_v),
        ("route", route_h, route_v), ("rw", rw_h, rw_v), ("pool", pool_h, pool_v),
        ("map", map_h.at[pl.ds(t * map_v.shape[0], map_v.shape[0])], map_v),
        ("scale", scale_h.at[:, pl.ds(pl.multiple_of(t * scale_v.shape[1], 128), scale_v.shape[1])], scale_v),
        ("sg", sg_h, sg_v), ("su", su_h, su_v), ("sd", sd_h, sd_v), ("proj", proj_h, proj_v),
        ("gate", gate_h.at[0], gate_v), ("up", up_h.at[0], up_v), ("down", down_h.at[0], down_v),
    )):
        cp = pltpu.make_async_copy(src, dst, load_sem.at[i])
        cp.start()
        loads[name] = cp

    sent = []

    def remote(src, dst, ssem, rsem, ep, tp):
        return pltpu.make_async_remote_copy(src_ref=src, dst_ref=dst, send_sem=ssem, recv_sem=rsem,
                                            device_id={"ep": ep, "tp": tp},
                                            device_id_type=pl.DeviceIdType.MESH)

    def start(cp):
        cp.start()
        sent.append(cp)

    def push(src, dst, ssem, rsem, ep, tp):
        start(remote(src, dst, ssem, rsem, ep, tp))

    def arrived(ref, ssem, rsem):
        pltpu.make_async_remote_copy(src_ref=ref, dst_ref=ref, send_sem=ssem, recv_sem=rsem,
                                     device_id={"ep": e, "tp": tc},
                                     device_id_type=pl.DeviceIdType.MESH).wait_recv()

    def routing(k):
        w = wts_v[k]
        a = lax.broadcasted_iota(jnp.int32, (toks, toks), 0)
        b = lax.broadcasted_iota(jnp.int32, (toks, toks), 1)
        before = jnp.where(a < b, 1.0, 0.0).astype(bf16)
        slot = jnp.dot(jnp.where(w > 0.0, 1.0, 0.0).astype(bf16), before, preferred_element_type=f32)
        slot_v[k] = jnp.where(w > 0.0, slot, -1024.0)
        own_row, other_row = slot_v[k, pl.ds(e, 1), :], slot_v[k, pl.ds(ex, 1), :]
        r = lax.broadcasted_iota(jnp.int32, (X_SIDE * cap, toks), 0).astype(f32)
        place = jnp.where(r < float(cap), jnp.broadcast_to(own_row, r.shape),
                          jnp.broadcast_to(other_row, r.shape) + float(cap))
        pick_v[k] = jnp.where(place == r, 1.0, 0.0).astype(bf16)

        def turned(row):
            return jnp.sum(jnp.where(a == b, jnp.broadcast_to(row, (toks, toks)), 0.0), axis=1, keepdims=True)

        s = lax.broadcasted_iota(jnp.int32, (toks, X_SIDE * cap), 1).astype(f32)
        first = s < float(cap)
        place = jnp.where(first, turned(own_row), turned(other_row) + float(cap))
        value = jnp.where(first, turned(wts_v[k, pl.ds(e, 1), :]), turned(wts_v[k, pl.ds(ex, 1), :]))
        mixw_v[k] = jnp.where(place == s, value, 0.0).astype(bf16)

    loads["moe"].wait()
    loads["gain"].wait()
    own = raw_row(0)

    def norm_step(i, carry):
        r = pl.multiple_of(i * 16, 16)
        v = moe_v[pl.ds(r, 16), :].astype(f32)
        cen = v - jnp.mean(v, axis=1, keepdims=True)
        var = jnp.mean(cen * cen, axis=1, keepdims=True)
        raw_v[pl.ds(own + r, 16), :] = (cen * lax.rsqrt(var + eps) * gain_v[...]).astype(bf16)
        return carry

    lax.fori_loop(0, toks // 16, norm_step, 0, unroll=2)
    loads["pool"].wait()
    loads["route"].wait()
    loads["rw"].wait()
    ids = lax.broadcasted_iota(jnp.int32, (n_ep, toks), 0)
    weights = jnp.zeros((n_ep, toks), f32)
    for top_step in range(route_v.shape[0]):
        named = jnp.broadcast_to(route_v[top_step:top_step + 1, :], (n_ep, toks)) == ids
        weights = weights + jnp.where(named, jnp.broadcast_to(rw_v[top_step:top_step + 1, :], (n_ep, toks)), 0.0)
    wts_v[0] = weights

    pl.semaphore_wait(barrier, n_ep - 1 + 2)

    for k in range(1, Z_SIDE):
        push(wts_v.at[0], wts_v.at[k], w_send.at[k], w_recv.at[k], kin[k] * X_SIDE + x, t)

    count = pool_v.shape[0]
    tail_ref = pool_v.at[pl.ds(count - HALO, HALO), :]

    def halo_copy(target):
        return pltpu.make_async_remote_copy(src_ref=tail_ref, dst_ref=halo_v, send_sem=halo_sem.at[0],
                                            recv_sem=halo_sem.at[1], device_id={"ep": target, "tp": t},
                                            device_id_type=pl.DeviceIdType.MESH)

    @pl.when(e < n_ep - 1)
    def _():
        halo_copy(e + 1).start()

    def spans():
        return ((col(t), part), (col(ty, near), rest))

    def raw_ref(k, i):
        c0, n = spans()[i]
        return raw_v.at[pl.ds(pl.multiple_of(kin[k] * toks, toks), toks), pl.ds(c0, n)]

    handed = []

    def hop(k, to, at, slot, i):
        return pltpu.make_async_remote_copy(
            src_ref=raw_ref(k, i), dst_ref=raw_ref(k, i), send_sem=z_send.at[slot, i], recv_sem=z_recv.at[at, i],
            device_id={"ep": kin[to] * X_SIDE + x, "tp": t}, device_id_type=pl.DeviceIdType.MESH)

    def hand(k, to, at, slot, i):
        handed.append((k, to, at, slot, i))
        hop(k, to, at, slot, i).start()

    for i in (0, 1):
        cp = hop(0, 1, 1, 0, i)
        cp.start()
        sent.append(cp)

        @pl.when(inner)
        def _():
            hand(0, 3, 3, 1, i)

    step = 256

    def gather(k, i):
        c0, n = spans()[i]
        for q in range(n // step):
            cq = pl.ds(pl.multiple_of(c0 + q * step, 128), step)
            o = jnp.dot(pick_v[turn[k]], raw_v[pl.ds(raw_row(k), toks), cq], preferred_element_type=f32).astype(bf16)
            comp_v[pl.ds(row0(k, 0), cap), cq] = o[:cap]
            xs_v[k * cap:(k + 1) * cap, cq] = o[cap:]

    def x_copy(k, i):
        c0, n = spans()[i]
        return remote(xs_v.at[k * cap:(k + 1) * cap, pl.ds(c0, n)], comp_v.at[pl.ds(row0(k, 0), cap), pl.ds(c0, n)],
                      x_send.at[k, i], x_recv.at[k, i], ex, t)

    def x_push(k, i):
        start(x_copy(k, i))

    def near_ref(k, j, s):
        return comp_v.at[pl.ds(row0(k, j), cap), pl.ds(col(s), near)]

    def near_copy(k, j):
        return remote(near_ref(k, j, t), near_ref(k, j, t), y_send.at[k, j], y_recv.at[k, j], e, ty)

    def near_push(k, j):
        start(near_copy(k, j))

    routing(0)
    for i in (0, 1):
        gather(0, i)
        x_push(0, i)

    def gather_rest(c0, n):
        for q in range(n // step):
            cq = pl.ds(pl.multiple_of(c0 + q * step, 128), step)
            comp_v[pl.ds(row0(0, 0), cap), cq] = jnp.dot(
                pick_v[0, :cap], raw_v[pl.ds(own, toks), cq], preferred_element_type=f32).astype(bf16)

    gather_rest(col(ty), near)
    gather_rest(col(tc), part)
    gather_rest(col(tyc), part)

    def z_wait(k, i):
        arrived(raw_ref(k, i), z_send.at[k, i], z_recv.at[k, i])

    def w_arrive(k):
        arrived(wts_v.at[k], w_send.at[k], w_recv.at[k])
        routing(k)

    def rows_out(k, i):
        go = start if k < 3 else lambda cp: cp.start()
        gather(k, i)
        go(x_copy(k, i))
        if i == 0:
            go(near_copy(k, 0))

    def z_piece(k, i):
        if k < 3:
            z_wait(k, i)

            @pl.when(inner)
            def _():
                if k == 1:
                    hand(1, 3, 2, 2, i)
                    z_wait(3, i)
                    hand(3, 1, 2, 3, i)
                else:
                    hand(2, 1, 3, 4, i)

            rows_out(k, i)
        else:
            z_wait(3, i)
            rows_out(k, i)

    def early(i):
        @pl.when(inner)
        def _():
            if i:
                out_push(1)
            rows_out(3, i)

    def late(i):
        @pl.when(jnp.logical_not(inner))
        def _():
            z_piece(3, i)
            if i:
                out_push(1)

    def x_piece(k, i):
        c0, n = spans()[i]
        arrived(comp_v.at[pl.ds(row0(k, 1), cap), pl.ds(c0, n)], x_send.at[k, i], x_recv.at[k, i])
        if i == 0:
            near_push(k, 1)

    def span(u):
        if u < 3:
            return pair_row(u), X_SIDE * cap
        return row0(3, u - 3), cap

    def part_ref(u, s):
        r, n = (row0(0, 1), cap) if u == 0 else span(u)
        return comp_v.at[pl.ds(r, n), pl.ds(col(s), part)]

    def y_arrive(u):
        k = min(u, 3)
        for j in (0, 1) if 0 < u < 3 else (1,) if u == 0 else (u - 3,):
            arrived(near_ref(k, j, ty), y_send.at[k, j], y_recv.at[k, j])
        for i, s in enumerate((t, ty)):
            push(part_ref(u, s), part_ref(u, s), c_send.at[u, i], c_recv.at[u, i], e, tc)

    def core_arrive(u):
        for i, s in enumerate((tc, tyc)):
            arrived(part_ref(u, s), c_send.at[u, i], c_recv.at[u, i])

    def hid_ref(u, s):
        r, n = span(u)
        return hid_v.at[pl.ds(r, n), pl.ds(pl.multiple_of(s * hid, 128), hid)]

    def expert_in(u):
        r, n = span(u)
        rows = comp_v[pl.ds(r, n), :]
        g = jnp.dot(rows, gate_v[...], preferred_element_type=f32)
        u_val = jnp.dot(rows, up_v[...], preferred_element_type=f32)
        hid_ref(u, t)[...] = (g / (1.0 + jnp.exp(-g)) * u_val).astype(bf16)
        push(hid_ref(u, t), hid_ref(u, t), h_send.at[u, 0], h_recv.at[u, 0], e, ty)
        push(hid_ref(u, t), hid_ref(u, t), h_send.at[u, 1], h_recv.at[u, 1], e, tc)

    def hid_forward(u):
        arrived(hid_ref(u, ty), h_send.at[u, 0], h_recv.at[u, 0])
        push(hid_ref(u, ty), hid_ref(u, ty), h_send.at[u, 2], h_recv.at[u, 2], e, tc)

    half = part // 2

    def half_copy(k, h):
        cols = pl.ds(h * half, half)
        return remote(outx_v.at[k, :, cols], pair_v.at[k, pl.ds(cap, cap), cols], rx_send.at[k, h],
                      rx_recv.at[k, h], ex, t)

    def half_push(k, h):
        go = start if k != 1 else lambda cp: cp.start()
        go(half_copy(k, h))

    def hid_wait(u):
        arrived(hid_ref(u, tc), h_send.at[u, 1], h_recv.at[u, 1])
        arrived(hid_ref(u, tyc), h_send.at[u, 2], h_recv.at[u, 2])

    def out_push(k):
        half_push(k, 0)
        half_push(k, 1)

    def expert_out(k, send=True):
        if k < 3:
            hid_wait(k)
        for j in (1, 0):
            if k == 3:
                hid_wait(3 + j)
            rows = hid_v[pl.ds(row0(k, j), cap), :]
            for q in range(part // 256):
                o = jnp.dot(rows, down_v[:, q * 256:(q + 1) * 256], preferred_element_type=f32).astype(bf16)
                if j:
                    outx_v[k, :, q * 256:(q + 1) * 256] = o
                    if send and (q + 1) * 256 % half == 0:
                        half_push(k, (q + 1) * 256 // half - 1)
                else:
                    pair_v[k, :cap, q * 256:(q + 1) * 256] = o

    def rz_copy(k, h):
        cols = pl.ds(h * half, half)
        return remote(part_send.at[k, :, cols], part_z.at[turn[k], :, cols], rz_send.at[k, h],
                      rz_recv.at[turn[k], h], zs[k] * X_SIDE + x, t)

    def sum_first(here):
        @pl.when(here)
        def _():
            sum_x(1)

    def sum_x(k):
        for h in (0, 1):
            cols = pl.ds(h * half, half)
            arrived(pair_v.at[k, pl.ds(cap, cap), cols], rx_send.at[k, h], rx_recv.at[k, h])
            both = jnp.dot(mixw_v[turn[k]], pair_v[k, :, cols], preferred_element_type=f32)
            if k:
                part_send[k, :, cols] = both.astype(bf16)
                go = start if k != 1 else lambda cp: cp.start()
                go(rz_copy(k, h))
            else:
                acc_v[:, cols] = both

    def shared():
        loads["sg"].wait()
        loads["su"].wait()
        rows = raw_v[pl.ds(own, toks), :]
        g = jnp.dot(rows, sg_v[...], preferred_element_type=f32)
        u = jnp.dot(rows, su_v[...], preferred_element_type=f32)
        shared_hidden = (g / (1.0 + jnp.exp(-g)) * u).astype(bf16)
        loads["sd"].wait()
        for q in range(width // 512):
            sh_v[:, q * 512:(q + 1) * 512] = jnp.dot(
                shared_hidden, sd_v[:, q * 512:(q + 1) * 512], preferred_element_type=f32).astype(bf16)
        for i, s in enumerate((tc, tyc)):
            push(sh_v.at[:, pl.ds(col(s), part)], sh_core.at[i], m_send.at[0, i], m_recv.at[0, i], e, tc)

    def pool():
        @pl.when(e == 0)
        def _():
            halo_v[...] = jnp.zeros_like(halo_v)

        @pl.when(e > 0)
        def _():
            halo_copy(e - 1).wait_recv()

        ext_v[:HALO, :] = halo_v[...].astype(f32)
        ext_v[HALO:, :] = pool_v[...].astype(f32)
        loads["map"].wait()
        loads["scale"].wait()
        dim = map_v.shape[1]
        position = (e * count + lax.broadcasted_iota(jnp.int32, (count, dim), 0)).astype(f32)
        for grp in range(map_v.shape[0]):
            w = windows[grp % 4]
            cs = slice(grp * dim, (grp + 1) * dim)
            values = ext_v[HALO:, cs]
            running = values
            for lag in range(1, w):
                running = running + ext_v[HALO - lag:HALO - lag + count, cs]
            pooled = (running / jnp.minimum(position + 1.0, float(w)) - values).astype(bf16)
            mapped = jnp.dot(pooled, map_v[grp], preferred_element_type=f32)
            group_v[:, cs] = (mapped * scale_v[:, cs]).astype(bf16)

    def proj():
        loads["proj"].wait()

        def proj_step(q, carry):
            cq = pl.ds(pl.multiple_of(q * 512, 512), 512)
            mix_v[:, cq] = jnp.dot(group_v[...], proj_v[:, cq], preferred_element_type=f32).astype(bf16)
            return carry

        lax.fori_loop(0, width // 512, proj_step, 0)
        for i, s in enumerate((tc, tyc)):
            push(mix_v.at[:, pl.ds(col(s), part)], mix_core.at[i], m_send.at[1, i], m_recv.at[1, i], e, tc)

    def core_sum(which, own_ref, core_ref, send_ref):
        for i in (0, 1):
            arrived(core_ref.at[i], m_send.at[which, i], m_recv.at[which, i])
        send_ref[...] = (own_ref[:, pl.ds(col(ty), part)].astype(f32) + core_ref[1].astype(f32)).astype(bf16)

    def sh_core_sum():
        core_sum(0, sh_v, sh_core, sh_send)

    def sh_push():
        push(sh_send, sh_y, m_send.at[0, 2], m_recv.at[0, 2], e, ty)

    def mix_core_sum():
        core_sum(1, mix_v, mix_core, mix_send)

    piece = count // MIX_PARTS

    def mix_push(n):
        push(mix_send.at[pl.ds(n * piece, piece)], mix_y.at[pl.ds(n * piece, piece)], ms_send.at[n], ms_recv.at[n],
             e, ty)

    def mix_final():
        for n in range(MIX_PARTS):
            arrived(mix_y.at[pl.ds(n * piece, piece)], ms_send.at[n], ms_recv.at[n])
        mix_out[...] = (mix_v[:, pl.ds(col(t), part)].astype(f32) + mix_core[0].astype(f32)
                        + mix_y[...].astype(f32)).astype(bf16)

    def sh_final():
        arrived(sh_y, m_send.at[0, 2], m_recv.at[0, 2])
        acc_v[...] = (acc_v[...] + sh_v[:, pl.ds(col(t), part)].astype(f32) + sh_core[0].astype(f32)
                      + sh_y[...].astype(f32))

    def z_final(h):
        cols = pl.ds(h * half, half)
        total = acc_v[:, cols]
        for k in (1, 2, 3):
            arrived(part_z.at[k, :, cols], rz_send.at[k, h], rz_recv.at[k, h])
            total = total + part_z[k, :, cols].astype(f32)
        moe_out[:, cols] = total.astype(bf16)

    def experts_loaded():
        loads["gate"].wait()
        loads["up"].wait()

    shared()
    w_arrive(1)
    w_arrive(2)
    w_arrive(3)
    pool()
    sh_core_sum()
    proj()
    x_piece(0, 0)
    mix_core_sum()
    z_piece(1, 0)
    x_piece(0, 1)
    z_piece(1, 1)
    y_arrive(0)
    x_piece(1, 0)
    core_arrive(0)
    experts_loaded()
    expert_in(0)
    z_piece(2, 0)
    x_piece(1, 1)
    y_arrive(1)
    core_arrive(1)
    expert_in(1)
    z_piece(2, 1)
    early(0)
    hid_forward(0)
    x_piece(2, 0)
    loads["down"].wait()
    expert_out(0, False)
    hid_forward(1)
    x_piece(2, 1)
    y_arrive(2)
    late(0)
    expert_out(1, False)
    early(1)
    core_arrive(2)
    expert_in(2)
    late(1)
    y_arrive(3)
    x_piece(3, 0)
    hid_forward(2)
    core_arrive(3)
    sum_first(inner)
    expert_in(3)
    expert_out(2)
    x_piece(3, 1)
    y_arrive(4)
    hid_forward(3)
    core_arrive(4)
    expert_in(4)
    sh_push()
    mix_push(0)
    mix_push(1)
    mix_push(2)
    mix_push(3)
    sum_first(jnp.logical_not(inner))
    hid_forward(4)
    sum_x(2)
    expert_out(3)
    sum_x(3)
    out_push(0)
    sum_x(0)
    sh_final()
    mix_final()
    z_final(0)
    z_final(1)

    for cp in sent:
        cp.wait_send()
    for i in (0, 1):
        x_copy(3, i).wait_send()
        half_copy(1, i).wait_send()
        rz_copy(1, i).wait_send()
    near_copy(3, 0).wait_send()

    @pl.when(inner)
    def _():
        for which in handed:
            hop(*which).wait_send()

    @pl.when(e < n_ep - 1)
    def _():
        halo_copy(e + 1).wait_send()


NEAR = 2


def per_device_fused(
    pool_input, pool_map, pool_scale, out_proj, moe_input, norm_gain, routes, route_weights,
    expert_gate, expert_up, expert_down, shared_gate, shared_up, shared_down,
):
    f32, bf16 = jnp.float32, jnp.bfloat16
    n_ep = lax.axis_size("ep")
    toks, width = moe_input.shape
    top_count = routes.shape[1]
    count, channels = pool_input.shape
    dim = pool_map.shape[1]
    part = width // lax.axis_size("tp")
    cap = (3 * toks * top_count + 2 * n_ep - 1) // (2 * n_ep)
    dma = pltpu.SemaphoreType.DMA
    return pl.pallas_call(
        fused_kernel,
        out_shape=(pltpu.VMEM((count, part), bf16), pltpu.VMEM((toks, part), bf16)),
        in_specs=[pl.BlockSpec(memory_space=pl.ANY)] * 14,
        out_specs=(pl.BlockSpec(memory_space=pltpu.VMEM), pl.BlockSpec(memory_space=pltpu.VMEM)),
        scratch_shapes=[
            pltpu.VMEM((count, channels), bf16),
            pltpu.VMEM((channels // dim, dim, dim), bf16),
            pltpu.VMEM((1, channels), f32),
            pltpu.VMEM(out_proj.shape, bf16),
            pltpu.VMEM((toks, width), bf16),
            pltpu.VMEM((1, width), f32),
            pltpu.VMEM((top_count, toks), jnp.int32),
            pltpu.VMEM((top_count, toks), f32),
            pltpu.VMEM(expert_gate.shape[1:], bf16),
            pltpu.VMEM(expert_up.shape[1:], bf16),
            pltpu.VMEM(expert_down.shape[1:], bf16),
            pltpu.VMEM(shared_gate.shape, bf16),
            pltpu.VMEM(shared_up.shape, bf16),
            pltpu.VMEM(shared_down.shape, bf16),
            pltpu.VMEM((HALO, channels), bf16),
            pltpu.VMEM((HALO + count, channels), f32),
            pltpu.VMEM((count, channels), bf16),
            pltpu.VMEM((count, width), bf16),
            pltpu.VMEM((2, count, part), bf16),
            pltpu.VMEM((count, part), bf16),
            pltpu.VMEM((count, part), bf16),
            pltpu.VMEM((Z_SIDE * toks, width), bf16),
            pltpu.VMEM((n_ep * cap, width), bf16),
            pltpu.VMEM((Z_SIDE * cap, width), bf16),
            pltpu.VMEM((Z_SIDE, n_ep, toks), f32),
            pltpu.VMEM((Z_SIDE, n_ep, toks), f32),
            pltpu.VMEM((Z_SIDE, X_SIDE * cap, toks), bf16),
            pltpu.VMEM((Z_SIDE, toks, X_SIDE * cap), bf16),
            pltpu.VMEM((n_ep * cap, expert_down.shape[1]), bf16),
            pltpu.VMEM((Z_SIDE, cap, part), bf16),
            pltpu.VMEM((Z_SIDE, X_SIDE * cap, part), bf16),
            pltpu.VMEM((toks, part), f32),
            pltpu.VMEM((Z_SIDE, toks, part), bf16),
            pltpu.VMEM((Z_SIDE, toks, part), bf16),
            pltpu.VMEM((toks, width), bf16),
            pltpu.VMEM((2, toks, part), bf16),
            pltpu.VMEM((toks, part), bf16),
            pltpu.VMEM((toks, part), bf16),
            dma((14,)), dma((2,)),
            dma((5, 2)), dma((4, 2)), dma((4, 2)), dma((4, 2)), dma((4, 2)), dma((4, 2)),
            dma((5, 2)), dma((5, 2)), dma((4,)), dma((4,)), dma((5, 3)), dma((5, 3)),
            dma((4, 2)), dma((4, 2)), dma((4, 2)), dma((4, 2)), dma((2, 3)), dma((2, 3)),
            dma((MIX_PARTS,)), dma((MIX_PARTS,)),
        ],
        compiler_params=pltpu.CompilerParams(
            collective_id=0, has_side_effects=True, vmem_limit_bytes=60 * 1024 * 1024),
    )(
        pool_input, pool_map, pool_scale.reshape(1, -1), out_proj, moe_input, norm_gain.reshape(1, -1),
        routes.T, route_weights.T, expert_gate, expert_up, expert_down, shared_gate, shared_up, shared_down,
    )


def solution(mesh):
    plane = mesh.shape["ep"] == Z_SIDE * X_SIDE and mesh.shape["tp"] == Y_SIDE * CORES
    body = per_device_fused if plane else per_device
    return jax.shard_map(
        body,
        mesh=mesh,
        in_specs=(
            P("ep", "tp"),
            P(),
            P(),
            P("tp", None),
            P("ep", None),
            P(),
            P("ep", None),
            P("ep", None),
            P("ep", None, "tp"),
            P("ep", None, "tp"),
            P("ep", None, "tp"),
            P(None, "tp"),
            P(None, "tp"),
            P("tp", None),
        ),
        out_specs=(P("ep", "tp"), P("ep", "tp")),
        check_vma=False,
    )
```

```python
import jax
import jax.numpy as jnp
from jax import lax
from jax.experimental import pallas as pl
from jax.experimental.pallas import tpu as pltpu
from jax.sharding import PartitionSpec as P

windows = (2, 4, 8, 16)
reach_back = 15
eps = 1e-05


def passed_along(block, axis, distance):
    devices = range(lax.axis_size(axis))
    route = [(i - distance, i) for i in devices if i - distance in devices]
    return lax.ppermute(block, axis, route)


def pool_branch(pool_input, pool_map, pool_scale, out_proj):
    row_count = pool_input.shape[0]
    channels = pool_input.shape[1]
    group_dim = pool_map.shape[1]
    local_groups = channels // group_dim
    tp_rank = lax.axis_index("tp")
    ep_rank = lax.axis_index("ep")
    earlier_rows = passed_along(pool_input[row_count - reach_back :], "ep", 1)
    values = pool_input.astype(jnp.float32)
    extended = jnp.concatenate([earlier_rows.astype(jnp.float32), values], axis=0)
    position = (ep_rank * row_count + jnp.arange(row_count, dtype=jnp.int32)).astype(jnp.float32)
    group_ids = tp_rank * local_groups + jnp.arange(channels, dtype=jnp.int32) // group_dim
    group_kind = group_ids % 4
    running = jnp.zeros((row_count, channels), jnp.float32)
    pooled = -values
    for lag_step in range(reach_back + 1):
        running = running + extended[reach_back - lag_step : reach_back - lag_step + row_count]
        if lag_step + 1 in windows:
            kind_id = windows.index(lag_step + 1)
            counts = jnp.minimum(position + 1.0, float(lag_step + 1))
            select = (group_kind == kind_id).astype(jnp.float32)
            pooled = pooled + select[None, :] * running / counts[:, None]
    pooled = pooled.astype(jnp.bfloat16)
    my_maps = lax.dynamic_slice_in_dim(pool_map, tp_rank * local_groups, local_groups, 0)
    my_scale = lax.dynamic_slice_in_dim(pool_scale, tp_rank * channels, channels, 0)
    mapped = jnp.einsum(
        "rgc,gcd->rgd",
        pooled.reshape(row_count, local_groups, group_dim),
        my_maps,
        preferred_element_type=jnp.float32,
    )
    group_out = (mapped.reshape(row_count, channels) * my_scale[None, :]).astype(jnp.bfloat16)
    return jnp.dot(group_out, out_proj, preferred_element_type=jnp.float32)


def dispatch_rows(routes, expert_count, capacity):
    tok_count, top_count = routes.shape
    flat_ids = routes.reshape(tok_count * top_count)
    one_hot = (flat_ids[:, None] == jnp.arange(expert_count, dtype=jnp.int32)[None, :]).astype(
        jnp.int32
    )
    earlier = jnp.cumsum(one_hot, axis=0) - one_hot
    slot_ids = jnp.sum(earlier * one_hot, axis=1)
    return (flat_ids * capacity + slot_ids).reshape(tok_count, top_count)


def per_device(
    pool_input,
    pool_map,
    pool_scale,
    out_proj,
    moe_input,
    norm_gain,
    routes,
    route_weights,
    expert_gate,
    expert_up,
    expert_down,
    shared_gate,
    shared_up,
    shared_down,
):
    mixer_part = pool_branch(pool_input, pool_map, pool_scale, out_proj)
    values = moe_input.astype(jnp.float32)
    centre = values - jnp.mean(values, axis=1, keepdims=True)
    variance = jnp.mean(centre * centre, axis=1, keepdims=True)
    normed = (centre * lax.rsqrt(variance + eps) * norm_gain[None, :]).astype(jnp.bfloat16)
    expert_count = lax.axis_size("ep")
    tok_count = moe_input.shape[0]
    top_count = routes.shape[1]
    capacity = (3 * tok_count * top_count + 2 * expert_count - 1) // (2 * expert_count)
    slot_index = dispatch_rows(routes, expert_count, capacity)
    buffer_len = expert_count * capacity
    targets = jnp.arange(buffer_len, dtype=jnp.int32)[:, None]
    placing = jnp.zeros((buffer_len, tok_count), jnp.float32)
    for top_step in range(top_count):
        placing = placing + (targets == slot_index[None, :, top_step]).astype(jnp.float32)
    outgoing = jnp.dot(
        placing.astype(jnp.bfloat16), normed, preferred_element_type=jnp.float32
    ).astype(jnp.bfloat16)
    gate_weight = expert_gate[0]
    up_weight = expert_up[0]
    down_weight = expert_down[0]
    tp_rank = lax.axis_index("tp")
    slice_width = outgoing.shape[1] // lax.axis_size("tp")
    my_slice = lax.dynamic_slice_in_dim(outgoing, tp_rank * slice_width, slice_width, 1)
    arrived = lax.all_to_all(my_slice, "ep", split_axis=0, concat_axis=0, tiled=True)
    shard_cols = lax.all_gather(arrived, "tp", axis=1, tiled=True)
    gate_val = jnp.dot(shard_cols, gate_weight, preferred_element_type=jnp.float32)
    up_val = jnp.dot(shard_cols, up_weight, preferred_element_type=jnp.float32)
    hidden = (jax.nn.silu(gate_val) * up_val).astype(jnp.bfloat16)
    expert_result = jnp.dot(
        lax.all_gather(hidden, "tp", axis=1, tiled=True),
        down_weight,
        preferred_element_type=jnp.float32,
    ).astype(jnp.bfloat16)
    returned = lax.all_to_all(expert_result, "ep", split_axis=0, concat_axis=0, tiled=True)
    routed = jnp.zeros((tok_count, returned.shape[1]), jnp.float32)
    for top_step in range(top_count):
        picked = returned[slot_index[:, top_step]].astype(jnp.float32)
        routed = routed + route_weights[:, top_step, None] * picked
    shared_gate_val = jnp.dot(normed, shared_gate, preferred_element_type=jnp.float32)
    shared_up_val = jnp.dot(normed, shared_up, preferred_element_type=jnp.float32)
    shared_hidden = (jax.nn.silu(shared_gate_val) * shared_up_val).astype(jnp.bfloat16)
    shared_part = jnp.dot(shared_hidden, shared_down, preferred_element_type=jnp.float32)
    mixer_sum, shared_sum = (
        lax.psum_scatter(
            mixer_part.astype(jnp.bfloat16), "tp", scatter_dimension=1, tiled=True
        ).astype(jnp.float32),
        lax.psum_scatter(
            shared_part.astype(jnp.bfloat16), "tp", scatter_dimension=1, tiled=True
        ).astype(jnp.float32),
    )
    return (mixer_sum.astype(jnp.bfloat16), (routed + shared_sum).astype(jnp.bfloat16))


HALO = 16
Z_SIDE, X_SIDE, Y_SIDE, CORES = 4, 2, 2, 2
MIX_PARTS = 4


def fused_kernel(
    pool_h, map_h, scale_h, proj_h, moe_h, gain_h, route_h, rw_h, gate_h, up_h, down_h, sg_h, su_h, sd_h,
    mix_out, moe_out,
    pool_v, map_v, scale_v, proj_v, moe_v, gain_v, route_v, rw_v, gate_v, up_v, down_v, sg_v, su_v, sd_v,
    halo_v, ext_v, group_v, mix_v, mix_core, mix_y, mix_send,
    raw_v, comp_v, xs_v, wts_v, slot_v, pick_v, mixw_v, hid_v, outx_v, pair_v, acc_v, part_z, part_send,
    sh_v, sh_core, sh_y, sh_send,
    load_sem, halo_sem, z_send, z_recv, x_send, x_recv, y_send, y_recv, c_send, c_recv,
    w_send, w_recv, h_send, h_recv, rx_send, rx_recv, rz_send, rz_recv, m_send, m_recv, ms_send, ms_recv,
):
    f32, bf16 = jnp.float32, jnp.bfloat16
    e = lax.axis_index("ep")
    t = lax.axis_index("tp")
    n_ep = Z_SIDE * X_SIDE
    z, x = e // X_SIDE, e % X_SIDE
    y, c = t // CORES, t % CORES
    toks = moe_h.shape[0]
    width = moe_h.shape[1]
    cap = comp_v.shape[0] // n_ep
    part = width // (Y_SIDE * CORES)
    hid = gate_h.shape[2]
    near = NEAR * part // 8
    rest = part - near
    inner = (z > 0) & (z < Z_SIDE - 1)
    kin = [z, z + 1 - 2 * (z % 2), (z + 2) % 4, 3 - z]
    turn = [0, jnp.where(inner, 3, 1), 2, jnp.where(inner, 1, 3)]
    zs = [z, jnp.where(inner, kin[3], kin[1]), kin[2], jnp.where(inner, kin[1], kin[3])]
    xs = [x, 1 - x]
    ex = z * X_SIDE + xs[1]
    ty, tc, tyc = (1 - y) * CORES + c, y * CORES + 1 - c, (1 - y) * CORES + 1 - c

    barrier = pltpu.get_barrier_semaphore()
    for k in range(Z_SIDE):
        for j in range(X_SIDE):
            if k or j:
                pl.semaphore_signal(barrier, inc=1, device_id={"ep": zs[k] * X_SIDE + xs[j], "tp": t},
                                    device_id_type=pl.DeviceIdType.MESH)
    for peer in (ty, tc):
        pl.semaphore_signal(barrier, inc=1, device_id={"ep": e, "tp": peer},
                            device_id_type=pl.DeviceIdType.MESH)

    def raw_row(k):
        return pl.multiple_of(zs[k] * toks, toks)

    def row0(k, j):
        return pl.multiple_of((zs[k] * X_SIDE + xs[j]) * cap, cap)

    def pair_row(k):
        return pl.multiple_of(zs[k] * X_SIDE * cap, X_SIDE * cap)

    def col(s, shift=0):
        return pl.multiple_of(s * part + shift, 128)

    loads = {}
    for i, (name, src, dst) in enumerate((
        ("moe", moe_h, moe_v), ("gain", gain_h, gain_v),
        ("route", route_h, route_v), ("rw", rw_h, rw_v), ("pool", pool_h, pool_v),
        ("map", map_h.at[pl.ds(t * map_v.shape[0], map_v.shape[0])], map_v),
        ("scale", scale_h.at[:, pl.ds(pl.multiple_of(t * scale_v.shape[1], 128), scale_v.shape[1])], scale_v),
        ("sg", sg_h, sg_v), ("su", su_h, su_v), ("sd", sd_h, sd_v), ("proj", proj_h, proj_v),
        ("gate", gate_h.at[0], gate_v), ("up", up_h.at[0], up_v), ("down", down_h.at[0], down_v),
    )):
        cp = pltpu.make_async_copy(src, dst, load_sem.at[i])
        cp.start()
        loads[name] = cp

    sent = []

    def remote(src, dst, ssem, rsem, ep, tp):
        return pltpu.make_async_remote_copy(src_ref=src, dst_ref=dst, send_sem=ssem, recv_sem=rsem,
                                            device_id={"ep": ep, "tp": tp},
                                            device_id_type=pl.DeviceIdType.MESH)

    def start(cp):
        cp.start()
        sent.append(cp)

    def push(src, dst, ssem, rsem, ep, tp):
        start(remote(src, dst, ssem, rsem, ep, tp))

    def arrived(ref, ssem, rsem):
        pltpu.make_async_remote_copy(src_ref=ref, dst_ref=ref, send_sem=ssem, recv_sem=rsem,
                                     device_id={"ep": e, "tp": tc},
                                     device_id_type=pl.DeviceIdType.MESH).wait_recv()

    def routing(k):
        w = wts_v[k]
        a = lax.broadcasted_iota(jnp.int32, (toks, toks), 0)
        b = lax.broadcasted_iota(jnp.int32, (toks, toks), 1)
        before = jnp.where(a < b, 1.0, 0.0).astype(bf16)
        slot = jnp.dot(jnp.where(w > 0.0, 1.0, 0.0).astype(bf16), before, preferred_element_type=f32)
        slot_v[k] = jnp.where(w > 0.0, slot, -1024.0)
        own_row, other_row = slot_v[k, pl.ds(e, 1), :], slot_v[k, pl.ds(ex, 1), :]
        r = lax.broadcasted_iota(jnp.int32, (X_SIDE * cap, toks), 0).astype(f32)
        place = jnp.where(r < float(cap), jnp.broadcast_to(own_row, r.shape),
                          jnp.broadcast_to(other_row, r.shape) + float(cap))
        pick_v[k] = jnp.where(place == r, 1.0, 0.0).astype(bf16)

        def turned(row):
            return jnp.sum(jnp.where(a == b, jnp.broadcast_to(row, (toks, toks)), 0.0), axis=1, keepdims=True)

        s = lax.broadcasted_iota(jnp.int32, (toks, X_SIDE * cap), 1).astype(f32)
        first = s < float(cap)
        place = jnp.where(first, turned(own_row), turned(other_row) + float(cap))
        value = jnp.where(first, turned(wts_v[k, pl.ds(e, 1), :]), turned(wts_v[k, pl.ds(ex, 1), :]))
        mixw_v[k] = jnp.where(place == s, value, 0.0).astype(bf16)

    loads["moe"].wait()
    loads["gain"].wait()
    own = raw_row(0)

    def norm_step(i, carry):
        r = pl.multiple_of(i * 16, 16)
        v = moe_v[pl.ds(r, 16), :].astype(f32)
        cen = v - jnp.mean(v, axis=1, keepdims=True)
        var = jnp.mean(cen * cen, axis=1, keepdims=True)
        raw_v[pl.ds(own + r, 16), :] = (cen * lax.rsqrt(var + eps) * gain_v[...]).astype(bf16)
        return carry

    lax.fori_loop(0, toks // 16, norm_step, 0, unroll=2)
    loads["pool"].wait()
    loads["route"].wait()
    loads["rw"].wait()
    ids = lax.broadcasted_iota(jnp.int32, (n_ep, toks), 0)
    weights = jnp.zeros((n_ep, toks), f32)
    for top_step in range(route_v.shape[0]):
        named = jnp.broadcast_to(route_v[top_step:top_step + 1, :], (n_ep, toks)) == ids
        weights = weights + jnp.where(named, jnp.broadcast_to(rw_v[top_step:top_step + 1, :], (n_ep, toks)), 0.0)
    wts_v[0] = weights

    pl.semaphore_wait(barrier, n_ep - 1 + 2)

    for k in range(1, Z_SIDE):
        push(wts_v.at[0], wts_v.at[k], w_send.at[k], w_recv.at[k], kin[k] * X_SIDE + x, t)

    count = pool_v.shape[0]
    tail_ref = pool_v.at[pl.ds(count - HALO, HALO), :]

    def halo_copy(target):
        return pltpu.make_async_remote_copy(src_ref=tail_ref, dst_ref=halo_v, send_sem=halo_sem.at[0],
                                            recv_sem=halo_sem.at[1], device_id={"ep": target, "tp": t},
                                            device_id_type=pl.DeviceIdType.MESH)

    @pl.when(e < n_ep - 1)
    def _():
        halo_copy(e + 1).start()

    def spans():
        return ((col(t), near), (col(t, near), rest), (col(ty, near), rest))

    def raw_ref(k, i):
        c0, n = spans()[i]
        return raw_v.at[pl.ds(pl.multiple_of(kin[k] * toks, toks), toks), pl.ds(c0, n)]

    handed = []

    def hop(k, to, at, slot, i):
        return pltpu.make_async_remote_copy(
            src_ref=raw_ref(k, i), dst_ref=raw_ref(k, i), send_sem=z_send.at[slot, i], recv_sem=z_recv.at[at, i],
            device_id={"ep": kin[to] * X_SIDE + x, "tp": t}, device_id_type=pl.DeviceIdType.MESH)

    def hand(k, to, at, slot, i):
        handed.append((k, to, at, slot, i))
        hop(k, to, at, slot, i).start()

    for i in range(3):
        cp = hop(0, 1, 1, 0, i)
        cp.start()
        sent.append(cp)

        @pl.when(inner)
        def _():
            hand(0, 3, 3, 1, i)

    step = 256

    def gather(k, i):
        c0, n = spans()[i]
        for q in range(n // step):
            cq = pl.ds(pl.multiple_of(c0 + q * step, 128), step)
            o = jnp.dot(pick_v[turn[k]], raw_v[pl.ds(raw_row(k), toks), cq], preferred_element_type=f32).astype(bf16)
            comp_v[pl.ds(row0(k, 0), cap), cq] = o[:cap]
            xs_v[k * cap:(k + 1) * cap, cq] = o[cap:]

    def x_copy(k, i):
        c0, n = spans()[i]
        return remote(xs_v.at[k * cap:(k + 1) * cap, pl.ds(c0, n)], comp_v.at[pl.ds(row0(k, 0), cap), pl.ds(c0, n)],
                      x_send.at[k, i], x_recv.at[k, i], ex, t)

    def x_push(k, i):
        start(x_copy(k, i))

    def near_ref(k, j, s):
        return comp_v.at[pl.ds(row0(k, j), cap), pl.ds(col(s), near)]

    def near_copy(k, j):
        return remote(near_ref(k, j, t), near_ref(k, j, t), y_send.at[k, j], y_recv.at[k, j], e, ty)

    def near_push(k, j):
        start(near_copy(k, j))

    routing(0)
    for i in range(3):
        gather(0, i)
        x_push(0, i)

    def gather_rest(c0, n):
        for q in range(n // step):
            cq = pl.ds(pl.multiple_of(c0 + q * step, 128), step)
            comp_v[pl.ds(row0(0, 0), cap), cq] = jnp.dot(
                pick_v[0, :cap], raw_v[pl.ds(own, toks), cq], preferred_element_type=f32).astype(bf16)

    gather_rest(col(ty), near)
    gather_rest(col(tc), part)
    gather_rest(col(tyc), part)

    def z_wait(k, i):
        arrived(raw_ref(k, i), z_send.at[k, i], z_recv.at[k, i])

    def w_arrive(k):
        arrived(wts_v.at[k], w_send.at[k], w_recv.at[k])
        routing(k)

    def rows_out(k, i):
        go = start if k < 3 else lambda cp: cp.start()
        gather(k, i)
        go(x_copy(k, i))
        if i == 0:
            go(near_copy(k, 0))

    def z_piece(k, i):
        if k < 3:
            z_wait(k, i)

            @pl.when(inner)
            def _():
                if k == 1:
                    hand(1, 3, 2, 2, i)
                    z_wait(3, i)
                    hand(3, 1, 2, 3, i)
                else:
                    hand(2, 1, 3, 4, i)

            rows_out(k, i)
        else:
            z_wait(3, i)
            rows_out(k, i)

    def early(i):
        @pl.when(inner)
        def _():
            if i == 2:
                out_push(1)
            rows_out(3, i)

    def late(i):
        @pl.when(jnp.logical_not(inner))
        def _():
            z_piece(3, i)
            if i == 2:
                out_push(1)

    def x_piece(k, i):
        c0, n = spans()[i]
        arrived(comp_v.at[pl.ds(row0(k, 1), cap), pl.ds(c0, n)], x_send.at[k, i], x_recv.at[k, i])
        if i == 0:
            near_push(k, 1)

    def span(u):
        if u < 3:
            return pair_row(u), X_SIDE * cap
        return row0(3, u - 3), cap

    def part_ref(u, s):
        r, n = (row0(0, 1), cap) if u == 0 else span(u)
        return comp_v.at[pl.ds(r, n), pl.ds(col(s), part)]

    def y_arrive(u):
        k = min(u, 3)
        for j in (0, 1) if 0 < u < 3 else (1,) if u == 0 else (u - 3,):
            arrived(near_ref(k, j, ty), y_send.at[k, j], y_recv.at[k, j])
        for i, s in enumerate((t, ty)):
            push(part_ref(u, s), part_ref(u, s), c_send.at[u, i], c_recv.at[u, i], e, tc)

    def core_arrive(u):
        for i, s in enumerate((tc, tyc)):
            arrived(part_ref(u, s), c_send.at[u, i], c_recv.at[u, i])

    def hid_ref(u, s):
        r, n = span(u)
        return hid_v.at[pl.ds(r, n), pl.ds(pl.multiple_of(s * hid, 128), hid)]

    def expert_in(u):
        r, n = span(u)
        rows = comp_v[pl.ds(r, n), :]
        g = jnp.dot(rows, gate_v[...], preferred_element_type=f32)
        u_val = jnp.dot(rows, up_v[...], preferred_element_type=f32)
        hid_ref(u, t)[...] = (g / (1.0 + jnp.exp(-g)) * u_val).astype(bf16)
        push(hid_ref(u, t), hid_ref(u, t), h_send.at[u, 0], h_recv.at[u, 0], e, ty)
        push(hid_ref(u, t), hid_ref(u, t), h_send.at[u, 1], h_recv.at[u, 1], e, tc)

    def hid_forward(u):
        arrived(hid_ref(u, ty), h_send.at[u, 0], h_recv.at[u, 0])
        push(hid_ref(u, ty), hid_ref(u, ty), h_send.at[u, 2], h_recv.at[u, 2], e, tc)

    half = part // 2

    def half_copy(k, h):
        cols = pl.ds(h * half, half)
        return remote(outx_v.at[k, :, cols], pair_v.at[k, pl.ds(cap, cap), cols], rx_send.at[k, h],
                      rx_recv.at[k, h], ex, t)

    def half_push(k, h):
        go = start if k != 1 else lambda cp: cp.start()
        go(half_copy(k, h))

    def hid_wait(u):
        arrived(hid_ref(u, tc), h_send.at[u, 1], h_recv.at[u, 1])
        arrived(hid_ref(u, tyc), h_send.at[u, 2], h_recv.at[u, 2])

    def out_push(k):
        half_push(k, 0)
        half_push(k, 1)

    def expert_out(k, send=True):
        if k < 3:
            hid_wait(k)
        for j in (1, 0):
            if k == 3:
                hid_wait(3 + j)
            rows = hid_v[pl.ds(row0(k, j), cap), :]
            for q in range(part // 256):
                o = jnp.dot(rows, down_v[:, q * 256:(q + 1) * 256], preferred_element_type=f32).astype(bf16)
                if j:
                    outx_v[k, :, q * 256:(q + 1) * 256] = o
                    if send and (q + 1) * 256 % half == 0:
                        half_push(k, (q + 1) * 256 // half - 1)
                else:
                    pair_v[k, :cap, q * 256:(q + 1) * 256] = o

    def rz_copy(k, h):
        cols = pl.ds(h * half, half)
        return remote(part_send.at[k, :, cols], part_z.at[turn[k], :, cols], rz_send.at[k, h],
                      rz_recv.at[turn[k], h], zs[k] * X_SIDE + x, t)

    def sum_when(k, here):
        @pl.when(here)
        def _():
            sum_x(k)

    def sum_x(k):
        for h in (0, 1):
            cols = pl.ds(h * half, half)
            arrived(pair_v.at[k, pl.ds(cap, cap), cols], rx_send.at[k, h], rx_recv.at[k, h])
            both = jnp.dot(mixw_v[turn[k]], pair_v[k, :, cols], preferred_element_type=f32)
            if k:
                part_send[k, :, cols] = both.astype(bf16)
                go = start if k == 3 else lambda cp: cp.start()
                go(rz_copy(k, h))
            else:
                acc_v[:, cols] = both

    def shared():
        loads["sg"].wait()
        loads["su"].wait()
        rows = raw_v[pl.ds(own, toks), :]
        g = jnp.dot(rows, sg_v[...], preferred_element_type=f32)
        u = jnp.dot(rows, su_v[...], preferred_element_type=f32)
        shared_hidden = (g / (1.0 + jnp.exp(-g)) * u).astype(bf16)
        loads["sd"].wait()
        for q in range(width // 512):
            sh_v[:, q * 512:(q + 1) * 512] = jnp.dot(
                shared_hidden, sd_v[:, q * 512:(q + 1) * 512], preferred_element_type=f32).astype(bf16)
        for i, s in enumerate((tc, tyc)):
            push(sh_v.at[:, pl.ds(col(s), part)], sh_core.at[i], m_send.at[0, i], m_recv.at[0, i], e, tc)

    def pool():
        @pl.when(e == 0)
        def _():
            halo_v[...] = jnp.zeros_like(halo_v)

        @pl.when(e > 0)
        def _():
            halo_copy(e - 1).wait_recv()

        ext_v[:HALO, :] = halo_v[...].astype(f32)
        ext_v[HALO:, :] = pool_v[...].astype(f32)
        loads["map"].wait()
        loads["scale"].wait()
        dim = map_v.shape[1]
        position = (e * count + lax.broadcasted_iota(jnp.int32, (count, dim), 0)).astype(f32)
        for grp in range(map_v.shape[0]):
            w = windows[grp % 4]
            cs = slice(grp * dim, (grp + 1) * dim)
            values = ext_v[HALO:, cs]
            running = values
            for lag in range(1, w):
                running = running + ext_v[HALO - lag:HALO - lag + count, cs]
            pooled = (running / jnp.minimum(position + 1.0, float(w)) - values).astype(bf16)
            mapped = jnp.dot(pooled, map_v[grp], preferred_element_type=f32)
            group_v[:, cs] = (mapped * scale_v[:, cs]).astype(bf16)

    def proj():
        loads["proj"].wait()

        def proj_step(q, carry):
            cq = pl.ds(pl.multiple_of(q * 512, 512), 512)
            mix_v[:, cq] = jnp.dot(group_v[...], proj_v[:, cq], preferred_element_type=f32).astype(bf16)
            return carry

        lax.fori_loop(0, width // 512, proj_step, 0)
        for i, s in enumerate((tc, tyc)):
            push(mix_v.at[:, pl.ds(col(s), part)], mix_core.at[i], m_send.at[1, i], m_recv.at[1, i], e, tc)

    def core_sum(which, own_ref, core_ref, send_ref):
        for i in (0, 1):
            arrived(core_ref.at[i], m_send.at[which, i], m_recv.at[which, i])
        send_ref[...] = (own_ref[:, pl.ds(col(ty), part)].astype(f32) + core_ref[1].astype(f32)).astype(bf16)

    def sh_core_sum():
        core_sum(0, sh_v, sh_core, sh_send)

    def sh_push():
        push(sh_send, sh_y, m_send.at[0, 2], m_recv.at[0, 2], e, ty)

    def mix_core_sum():
        core_sum(1, mix_v, mix_core, mix_send)

    piece = count // MIX_PARTS

    def mix_push(n):
        push(mix_send.at[pl.ds(n * piece, piece)], mix_y.at[pl.ds(n * piece, piece)], ms_send.at[n], ms_recv.at[n],
             e, ty)

    def mix_final():
        for n in range(MIX_PARTS):
            arrived(mix_y.at[pl.ds(n * piece, piece)], ms_send.at[n], ms_recv.at[n])
        mix_out[...] = (mix_v[:, pl.ds(col(t), part)].astype(f32) + mix_core[0].astype(f32)
                        + mix_y[...].astype(f32)).astype(bf16)

    def sh_final():
        arrived(sh_y, m_send.at[0, 2], m_recv.at[0, 2])
        acc_v[...] = (acc_v[...] + sh_v[:, pl.ds(col(t), part)].astype(f32) + sh_core[0].astype(f32)
                      + sh_y[...].astype(f32))

    def z_final(h):
        cols = pl.ds(h * half, half)
        total = acc_v[:, cols]
        for k in (1, 2, 3):
            arrived(part_z.at[k, :, cols], rz_send.at[k, h], rz_recv.at[k, h])
            total = total + part_z[k, :, cols].astype(f32)
        moe_out[:, cols] = total.astype(bf16)

    def experts_loaded():
        loads["gate"].wait()
        loads["up"].wait()

    outer = jnp.logical_not(inner)
    shared()
    w_arrive(1)
    w_arrive(2)
    w_arrive(3)
    pool()
    sh_core_sum()
    proj()
    x_piece(0, 0)
    z_piece(1, 0)
    x_piece(0, 1)
    mix_core_sum()
    z_piece(1, 1)
    x_piece(0, 2)
    y_arrive(0)
    z_piece(1, 2)
    x_piece(1, 0)
    core_arrive(0)
    experts_loaded()
    expert_in(0)
    z_piece(2, 0)
    x_piece(1, 1)
    x_piece(1, 2)
    y_arrive(1)
    z_piece(2, 1)
    x_piece(2, 0)
    core_arrive(1)
    expert_in(1)
    hid_forward(0)
    z_piece(2, 2)
    early(0)
    early(1)
    x_piece(2, 1)
    loads["down"].wait()
    expert_out(0, False)
    late(0)
    x_piece(2, 2)
    hid_forward(1)
    y_arrive(2)
    late(1)
    expert_out(1, False)
    early(2)
    core_arrive(2)
    x_piece(3, 0)
    expert_in(2)
    late(2)
    y_arrive(3)
    x_piece(3, 1)
    core_arrive(3)
    hid_forward(2)
    sum_when(1, inner)
    expert_in(3)
    x_piece(3, 2)
    y_arrive(4)
    expert_out(2)
    hid_forward(3)
    core_arrive(4)
    expert_in(4)
    sh_push()
    mix_push(0)
    mix_push(1)
    mix_push(2)
    mix_push(3)
    sum_when(1, outer)
    sum_when(2, inner)
    hid_forward(4)
    expert_out(3)
    sum_when(2, outer)
    sum_x(3)
    out_push(0)
    sum_x(0)
    sh_final()
    mix_final()
    z_final(0)
    z_final(1)

    for cp in sent:
        cp.wait_send()
    for i in range(3):
        x_copy(3, i).wait_send()
    for i in (0, 1):
        half_copy(1, i).wait_send()
        rz_copy(1, i).wait_send()
        rz_copy(2, i).wait_send()
    near_copy(3, 0).wait_send()

    @pl.when(inner)
    def _():
        for which in handed:
            hop(*which).wait_send()

    @pl.when(e < n_ep - 1)
    def _():
        halo_copy(e + 1).wait_send()


NEAR = 4


def per_device_fused(
    pool_input, pool_map, pool_scale, out_proj, moe_input, norm_gain, routes, route_weights,
    expert_gate, expert_up, expert_down, shared_gate, shared_up, shared_down,
):
    f32, bf16 = jnp.float32, jnp.bfloat16
    n_ep = lax.axis_size("ep")
    toks, width = moe_input.shape
    top_count = routes.shape[1]
    count, channels = pool_input.shape
    dim = pool_map.shape[1]
    part = width // lax.axis_size("tp")
    cap = (3 * toks * top_count + 2 * n_ep - 1) // (2 * n_ep)
    dma = pltpu.SemaphoreType.DMA
    return pl.pallas_call(
        fused_kernel,
        out_shape=(pltpu.VMEM((count, part), bf16), pltpu.VMEM((toks, part), bf16)),
        in_specs=[pl.BlockSpec(memory_space=pl.ANY)] * 14,
        out_specs=(pl.BlockSpec(memory_space=pltpu.VMEM), pl.BlockSpec(memory_space=pltpu.VMEM)),
        scratch_shapes=[
            pltpu.VMEM((count, channels), bf16),
            pltpu.VMEM((channels // dim, dim, dim), bf16),
            pltpu.VMEM((1, channels), f32),
            pltpu.VMEM(out_proj.shape, bf16),
            pltpu.VMEM((toks, width), bf16),
            pltpu.VMEM((1, width), f32),
            pltpu.VMEM((top_count, toks), jnp.int32),
            pltpu.VMEM((top_count, toks), f32),
            pltpu.VMEM(expert_gate.shape[1:], bf16),
            pltpu.VMEM(expert_up.shape[1:], bf16),
            pltpu.VMEM(expert_down.shape[1:], bf16),
            pltpu.VMEM(shared_gate.shape, bf16),
            pltpu.VMEM(shared_up.shape, bf16),
            pltpu.VMEM(shared_down.shape, bf16),
            pltpu.VMEM((HALO, channels), bf16),
            pltpu.VMEM((HALO + count, channels), f32),
            pltpu.VMEM((count, channels), bf16),
            pltpu.VMEM((count, width), bf16),
            pltpu.VMEM((2, count, part), bf16),
            pltpu.VMEM((count, part), bf16),
            pltpu.VMEM((count, part), bf16),
            pltpu.VMEM((Z_SIDE * toks, width), bf16),
            pltpu.VMEM((n_ep * cap, width), bf16),
            pltpu.VMEM((Z_SIDE * cap, width), bf16),
            pltpu.VMEM((Z_SIDE, n_ep, toks), f32),
            pltpu.VMEM((Z_SIDE, n_ep, toks), f32),
            pltpu.VMEM((Z_SIDE, X_SIDE * cap, toks), bf16),
            pltpu.VMEM((Z_SIDE, toks, X_SIDE * cap), bf16),
            pltpu.VMEM((n_ep * cap, expert_down.shape[1]), bf16),
            pltpu.VMEM((Z_SIDE, cap, part), bf16),
            pltpu.VMEM((Z_SIDE, X_SIDE * cap, part), bf16),
            pltpu.VMEM((toks, part), f32),
            pltpu.VMEM((Z_SIDE, toks, part), bf16),
            pltpu.VMEM((Z_SIDE, toks, part), bf16),
            pltpu.VMEM((toks, width), bf16),
            pltpu.VMEM((2, toks, part), bf16),
            pltpu.VMEM((toks, part), bf16),
            pltpu.VMEM((toks, part), bf16),
            dma((14,)), dma((2,)),
            dma((5, 3)), dma((5, 3)), dma((4, 3)), dma((4, 3)), dma((4, 2)), dma((4, 2)),
            dma((5, 2)), dma((5, 2)), dma((4,)), dma((4,)), dma((5, 3)), dma((5, 3)),
            dma((4, 2)), dma((4, 2)), dma((4, 2)), dma((4, 2)), dma((2, 3)), dma((2, 3)),
            dma((MIX_PARTS,)), dma((MIX_PARTS,)),
        ],
        compiler_params=pltpu.CompilerParams(
            collective_id=0, has_side_effects=True, vmem_limit_bytes=60 * 1024 * 1024),
    )(
        pool_input, pool_map, pool_scale.reshape(1, -1), out_proj, moe_input, norm_gain.reshape(1, -1),
        routes.T, route_weights.T, expert_gate, expert_up, expert_down, shared_gate, shared_up, shared_down,
    )


def solution(mesh):
    plane = mesh.shape["ep"] == Z_SIDE * X_SIDE and mesh.shape["tp"] == Y_SIDE * CORES
    body = per_device_fused if plane else per_device
    return jax.shard_map(
        body,
        mesh=mesh,
        in_specs=(
            P("ep", "tp"),
            P(),
            P(),
            P("tp", None),
            P("ep", None),
            P(),
            P("ep", None),
            P("ep", None),
            P("ep", None, "tp"),
            P("ep", None, "tp"),
            P("ep", None, "tp"),
            P(None, "tp"),
            P(None, "tp"),
            P("tp", None),
        ),
        out_specs=(P("ep", "tp"), P("ep", "tp")),
        check_vma=False,
    )
```

```python
import jax
import jax.numpy as jnp
from jax import lax
from jax.experimental import pallas as pl
from jax.experimental.pallas import tpu as pltpu
from jax.sharding import PartitionSpec as P

windows = (2, 4, 8, 16)
reach_back = 15
eps = 1e-05


def passed_along(block, axis, distance):
    devices = range(lax.axis_size(axis))
    route = [(i - distance, i) for i in devices if i - distance in devices]
    return lax.ppermute(block, axis, route)


def pool_branch(pool_input, pool_map, pool_scale, out_proj):
    row_count = pool_input.shape[0]
    channels = pool_input.shape[1]
    group_dim = pool_map.shape[1]
    local_groups = channels // group_dim
    tp_rank = lax.axis_index("tp")
    ep_rank = lax.axis_index("ep")
    earlier_rows = passed_along(pool_input[row_count - reach_back :], "ep", 1)
    values = pool_input.astype(jnp.float32)
    extended = jnp.concatenate([earlier_rows.astype(jnp.float32), values], axis=0)
    position = (ep_rank * row_count + jnp.arange(row_count, dtype=jnp.int32)).astype(jnp.float32)
    group_ids = tp_rank * local_groups + jnp.arange(channels, dtype=jnp.int32) // group_dim
    group_kind = group_ids % 4
    running = jnp.zeros((row_count, channels), jnp.float32)
    pooled = -values
    for lag_step in range(reach_back + 1):
        running = running + extended[reach_back - lag_step : reach_back - lag_step + row_count]
        if lag_step + 1 in windows:
            kind_id = windows.index(lag_step + 1)
            counts = jnp.minimum(position + 1.0, float(lag_step + 1))
            select = (group_kind == kind_id).astype(jnp.float32)
            pooled = pooled + select[None, :] * running / counts[:, None]
    pooled = pooled.astype(jnp.bfloat16)
    my_maps = lax.dynamic_slice_in_dim(pool_map, tp_rank * local_groups, local_groups, 0)
    my_scale = lax.dynamic_slice_in_dim(pool_scale, tp_rank * channels, channels, 0)
    mapped = jnp.einsum(
        "rgc,gcd->rgd",
        pooled.reshape(row_count, local_groups, group_dim),
        my_maps,
        preferred_element_type=jnp.float32,
    )
    group_out = (mapped.reshape(row_count, channels) * my_scale[None, :]).astype(jnp.bfloat16)
    return jnp.dot(group_out, out_proj, preferred_element_type=jnp.float32)


def dispatch_rows(routes, expert_count, capacity):
    tok_count, top_count = routes.shape
    flat_ids = routes.reshape(tok_count * top_count)
    one_hot = (flat_ids[:, None] == jnp.arange(expert_count, dtype=jnp.int32)[None, :]).astype(
        jnp.int32
    )
    earlier = jnp.cumsum(one_hot, axis=0) - one_hot
    slot_ids = jnp.sum(earlier * one_hot, axis=1)
    return (flat_ids * capacity + slot_ids).reshape(tok_count, top_count)


def per_device(
    pool_input,
    pool_map,
    pool_scale,
    out_proj,
    moe_input,
    norm_gain,
    routes,
    route_weights,
    expert_gate,
    expert_up,
    expert_down,
    shared_gate,
    shared_up,
    shared_down,
):
    mixer_part = pool_branch(pool_input, pool_map, pool_scale, out_proj)
    values = moe_input.astype(jnp.float32)
    centre = values - jnp.mean(values, axis=1, keepdims=True)
    variance = jnp.mean(centre * centre, axis=1, keepdims=True)
    normed = (centre * lax.rsqrt(variance + eps) * norm_gain[None, :]).astype(jnp.bfloat16)
    expert_count = lax.axis_size("ep")
    tok_count = moe_input.shape[0]
    top_count = routes.shape[1]
    capacity = (3 * tok_count * top_count + 2 * expert_count - 1) // (2 * expert_count)
    slot_index = dispatch_rows(routes, expert_count, capacity)
    buffer_len = expert_count * capacity
    targets = jnp.arange(buffer_len, dtype=jnp.int32)[:, None]
    placing = jnp.zeros((buffer_len, tok_count), jnp.float32)
    for top_step in range(top_count):
        placing = placing + (targets == slot_index[None, :, top_step]).astype(jnp.float32)
    outgoing = jnp.dot(
        placing.astype(jnp.bfloat16), normed, preferred_element_type=jnp.float32
    ).astype(jnp.bfloat16)
    gate_weight = expert_gate[0]
    up_weight = expert_up[0]
    down_weight = expert_down[0]
    tp_rank = lax.axis_index("tp")
    slice_width = outgoing.shape[1] // lax.axis_size("tp")
    my_slice = lax.dynamic_slice_in_dim(outgoing, tp_rank * slice_width, slice_width, 1)
    arrived = lax.all_to_all(my_slice, "ep", split_axis=0, concat_axis=0, tiled=True)
    shard_cols = lax.all_gather(arrived, "tp", axis=1, tiled=True)
    gate_val = jnp.dot(shard_cols, gate_weight, preferred_element_type=jnp.float32)
    up_val = jnp.dot(shard_cols, up_weight, preferred_element_type=jnp.float32)
    hidden = (jax.nn.silu(gate_val) * up_val).astype(jnp.bfloat16)
    expert_result = jnp.dot(
        lax.all_gather(hidden, "tp", axis=1, tiled=True),
        down_weight,
        preferred_element_type=jnp.float32,
    ).astype(jnp.bfloat16)
    returned = lax.all_to_all(expert_result, "ep", split_axis=0, concat_axis=0, tiled=True)
    routed = jnp.zeros((tok_count, returned.shape[1]), jnp.float32)
    for top_step in range(top_count):
        picked = returned[slot_index[:, top_step]].astype(jnp.float32)
        routed = routed + route_weights[:, top_step, None] * picked
    shared_gate_val = jnp.dot(normed, shared_gate, preferred_element_type=jnp.float32)
    shared_up_val = jnp.dot(normed, shared_up, preferred_element_type=jnp.float32)
    shared_hidden = (jax.nn.silu(shared_gate_val) * shared_up_val).astype(jnp.bfloat16)
    shared_part = jnp.dot(shared_hidden, shared_down, preferred_element_type=jnp.float32)
    mixer_sum, shared_sum = (
        lax.psum_scatter(
            mixer_part.astype(jnp.bfloat16), "tp", scatter_dimension=1, tiled=True
        ).astype(jnp.float32),
        lax.psum_scatter(
            shared_part.astype(jnp.bfloat16), "tp", scatter_dimension=1, tiled=True
        ).astype(jnp.float32),
    )
    return (mixer_sum.astype(jnp.bfloat16), (routed + shared_sum).astype(jnp.bfloat16))


HALO = 16
Z_SIDE, X_SIDE, Y_SIDE, CORES = 4, 2, 2, 2
MIX_PARTS = 4


def fused_kernel(
    pool_h, map_h, scale_h, proj_h, moe_h, gain_h, route_h, rw_h, gate_h, up_h, down_h, sg_h, su_h, sd_h,
    mix_out, moe_out,
    pool_v, map_v, scale_v, proj_v, moe_v, gain_v, route_v, rw_v, gate_v, up_v, down_v, sg_v, su_v, sd_v,
    halo_v, ext_v, group_v, mix_v, mix_core, mix_y, mix_send,
    raw_v, comp_v, xs_v, wts_v, slot_v, pick_v, mixw_v, hid_v, outx_v, pair_v, acc_v, part_z, part_send,
    sh_v, sh_core, sh_y, sh_send,
    load_sem, halo_sem, z_send, z_recv, x_send, x_recv, y_send, y_recv, c_send, c_recv,
    w_send, w_recv, h_send, h_recv, rx_send, rx_recv, rz_send, rz_recv, m_send, m_recv, ms_send, ms_recv,
):
    f32, bf16 = jnp.float32, jnp.bfloat16
    e = lax.axis_index("ep")
    t = lax.axis_index("tp")
    n_ep = Z_SIDE * X_SIDE
    z, x = e // X_SIDE, e % X_SIDE
    y, c = t // CORES, t % CORES
    toks = moe_h.shape[0]
    width = moe_h.shape[1]
    cap = comp_v.shape[0] // n_ep
    part = width // (Y_SIDE * CORES)
    hid = gate_h.shape[2]
    near = NEAR * part // 8
    rest = part - near
    inner = (z > 0) & (z < Z_SIDE - 1)
    kin = [z, z + 1 - 2 * (z % 2), (z + 2) % 4, 3 - z]
    turn = [0, jnp.where(inner, 3, 1), 2, jnp.where(inner, 1, 3)]
    zs = [z, jnp.where(inner, kin[3], kin[1]), kin[2], jnp.where(inner, kin[1], kin[3])]
    xs = [x, 1 - x]
    ex = z * X_SIDE + xs[1]
    ty, tc, tyc = (1 - y) * CORES + c, y * CORES + 1 - c, (1 - y) * CORES + 1 - c

    barrier = pltpu.get_barrier_semaphore()
    for k in range(Z_SIDE):
        for j in range(X_SIDE):
            if k or j:
                pl.semaphore_signal(barrier, inc=1, device_id={"ep": zs[k] * X_SIDE + xs[j], "tp": t},
                                    device_id_type=pl.DeviceIdType.MESH)
    for peer in (ty, tc):
        pl.semaphore_signal(barrier, inc=1, device_id={"ep": e, "tp": peer},
                            device_id_type=pl.DeviceIdType.MESH)

    def raw_row(k):
        return pl.multiple_of(zs[k] * toks, toks)

    def row0(k, j):
        return pl.multiple_of((zs[k] * X_SIDE + xs[j]) * cap, cap)

    def pair_row(k):
        return pl.multiple_of(zs[k] * X_SIDE * cap, X_SIDE * cap)

    def col(s, shift=0):
        return pl.multiple_of(s * part + shift, 128)

    loads = {}
    for i, (name, src, dst) in enumerate((
        ("moe", moe_h, moe_v), ("gain", gain_h, gain_v),
        ("route", route_h, route_v), ("rw", rw_h, rw_v), ("pool", pool_h, pool_v),
        ("map", map_h.at[pl.ds(t * map_v.shape[0], map_v.shape[0])], map_v),
        ("scale", scale_h.at[:, pl.ds(pl.multiple_of(t * scale_v.shape[1], 128), scale_v.shape[1])], scale_v),
        ("sg", sg_h, sg_v), ("su", su_h, su_v), ("sd", sd_h, sd_v), ("proj", proj_h, proj_v),
        ("gate", gate_h.at[0], gate_v), ("up", up_h.at[0], up_v), ("down", down_h.at[0], down_v),
    )):
        cp = pltpu.make_async_copy(src, dst, load_sem.at[i])
        cp.start()
        loads[name] = cp

    sent = []

    def remote(src, dst, ssem, rsem, ep, tp):
        return pltpu.make_async_remote_copy(src_ref=src, dst_ref=dst, send_sem=ssem, recv_sem=rsem,
                                            device_id={"ep": ep, "tp": tp},
                                            device_id_type=pl.DeviceIdType.MESH)

    def start(cp):
        cp.start()
        sent.append(cp)

    def push(src, dst, ssem, rsem, ep, tp):
        start(remote(src, dst, ssem, rsem, ep, tp))

    def arrived(ref, ssem, rsem):
        pltpu.make_async_remote_copy(src_ref=ref, dst_ref=ref, send_sem=ssem, recv_sem=rsem,
                                     device_id={"ep": e, "tp": tc},
                                     device_id_type=pl.DeviceIdType.MESH).wait_recv()

    def routing(k):
        w = wts_v[k]
        a = lax.broadcasted_iota(jnp.int32, (toks, toks), 0)
        b = lax.broadcasted_iota(jnp.int32, (toks, toks), 1)
        before = jnp.where(a < b, 1.0, 0.0).astype(bf16)
        slot = jnp.dot(jnp.where(w > 0.0, 1.0, 0.0).astype(bf16), before, preferred_element_type=f32)
        slot_v[k] = jnp.where(w > 0.0, slot, -1024.0)
        own_row, other_row = slot_v[k, pl.ds(e, 1), :], slot_v[k, pl.ds(ex, 1), :]
        r = lax.broadcasted_iota(jnp.int32, (X_SIDE * cap, toks), 0).astype(f32)
        place = jnp.where(r < float(cap), jnp.broadcast_to(own_row, r.shape),
                          jnp.broadcast_to(other_row, r.shape) + float(cap))
        pick_v[k] = jnp.where(place == r, 1.0, 0.0).astype(bf16)

        def turned(row):
            return jnp.sum(jnp.where(a == b, jnp.broadcast_to(row, (toks, toks)), 0.0), axis=1, keepdims=True)

        s = lax.broadcasted_iota(jnp.int32, (toks, X_SIDE * cap), 1).astype(f32)
        first = s < float(cap)
        place = jnp.where(first, turned(own_row), turned(other_row) + float(cap))
        value = jnp.where(first, turned(wts_v[k, pl.ds(e, 1), :]), turned(wts_v[k, pl.ds(ex, 1), :]))
        mixw_v[k] = jnp.where(place == s, value, 0.0).astype(bf16)

    loads["moe"].wait()
    loads["gain"].wait()
    own = raw_row(0)

    def norm_step(i, carry):
        r = pl.multiple_of(i * 16, 16)
        v = moe_v[pl.ds(r, 16), :].astype(f32)
        cen = v - jnp.mean(v, axis=1, keepdims=True)
        var = jnp.mean(cen * cen, axis=1, keepdims=True)
        raw_v[pl.ds(own + r, 16), :] = (cen * lax.rsqrt(var + eps) * gain_v[...]).astype(bf16)
        return carry

    lax.fori_loop(0, toks // 16, norm_step, 0, unroll=4)
    loads["pool"].wait()
    loads["route"].wait()
    loads["rw"].wait()
    ids = lax.broadcasted_iota(jnp.int32, (n_ep, toks), 0)
    weights = jnp.zeros((n_ep, toks), f32)
    for top_step in range(route_v.shape[0]):
        named = jnp.broadcast_to(route_v[top_step:top_step + 1, :], (n_ep, toks)) == ids
        weights = weights + jnp.where(named, jnp.broadcast_to(rw_v[top_step:top_step + 1, :], (n_ep, toks)), 0.0)
    wts_v[0] = weights

    pl.semaphore_wait(barrier, n_ep - 1 + 2)

    for k in range(1, Z_SIDE):
        push(wts_v.at[0], wts_v.at[k], w_send.at[k], w_recv.at[k], kin[k] * X_SIDE + x, t)

    count = pool_v.shape[0]
    tail_ref = pool_v.at[pl.ds(count - HALO, HALO), :]

    def halo_copy(target):
        return pltpu.make_async_remote_copy(src_ref=tail_ref, dst_ref=halo_v, send_sem=halo_sem.at[0],
                                            recv_sem=halo_sem.at[1], device_id={"ep": target, "tp": t},
                                            device_id_type=pl.DeviceIdType.MESH)

    @pl.when(e < n_ep - 1)
    def _():
        halo_copy(e + 1).start()

    def spans():
        return ((col(t), near), (col(t, near), rest), (col(ty, near), rest))

    def raw_ref(k, i):
        c0, n = spans()[i]
        return raw_v.at[pl.ds(pl.multiple_of(kin[k] * toks, toks), toks), pl.ds(c0, n)]

    handed = []

    def hop(k, to, at, slot, i):
        return pltpu.make_async_remote_copy(
            src_ref=raw_ref(k, i), dst_ref=raw_ref(k, i), send_sem=z_send.at[slot, i], recv_sem=z_recv.at[at, i],
            device_id={"ep": kin[to] * X_SIDE + x, "tp": t}, device_id_type=pl.DeviceIdType.MESH)

    def hand(k, to, at, slot, i):
        handed.append((k, to, at, slot, i))
        hop(k, to, at, slot, i).start()

    for i in range(3):
        cp = hop(0, 1, 1, 0, i)
        cp.start()
        sent.append(cp)

        @pl.when(inner)
        def _():
            hand(0, 3, 3, 1, i)

    step = 256

    def gather(k, i):
        c0, n = spans()[i]
        for q in range(n // step):
            cq = pl.ds(pl.multiple_of(c0 + q * step, 128), step)
            o = jnp.dot(pick_v[turn[k]], raw_v[pl.ds(raw_row(k), toks), cq], preferred_element_type=f32).astype(bf16)
            comp_v[pl.ds(row0(k, 0), cap), cq] = o[:cap]
            xs_v[k * cap:(k + 1) * cap, cq] = o[cap:]

    def x_copy(k, i):
        c0, n = spans()[i]
        return remote(xs_v.at[k * cap:(k + 1) * cap, pl.ds(c0, n)], comp_v.at[pl.ds(row0(k, 0), cap), pl.ds(c0, n)],
                      x_send.at[k, i], x_recv.at[k, i], ex, t)

    def x_push(k, i):
        start(x_copy(k, i))

    def near_ref(k, j, s):
        return comp_v.at[pl.ds(row0(k, j), cap), pl.ds(col(s), near)]

    def near_copy(k, j):
        return remote(near_ref(k, j, t), near_ref(k, j, t), y_send.at[k, j], y_recv.at[k, j], e, ty)

    def near_push(k, j):
        start(near_copy(k, j))

    routing(0)
    for i in range(3):
        gather(0, i)
        x_push(0, i)

    def gather_rest(c0, n):
        for q in range(n // step):
            cq = pl.ds(pl.multiple_of(c0 + q * step, 128), step)
            comp_v[pl.ds(row0(0, 0), cap), cq] = jnp.dot(
                pick_v[0, :cap], raw_v[pl.ds(own, toks), cq], preferred_element_type=f32).astype(bf16)

    gather_rest(col(ty), near)
    gather_rest(col(tc), part)
    gather_rest(col(tyc), part)

    def z_wait(k, i):
        arrived(raw_ref(k, i), z_send.at[k, i], z_recv.at[k, i])

    def w_arrive(k):
        arrived(wts_v.at[k], w_send.at[k], w_recv.at[k])
        routing(k)

    def rows_out(k, i):
        go = start if k < 3 else lambda cp: cp.start()
        gather(k, i)
        go(x_copy(k, i))

    def z_piece(k, i):
        if k < 3:
            z_wait(k, i)

            @pl.when(inner)
            def _():
                if k == 1:
                    hand(1, 3, 2, 2, i)
                    z_wait(3, i)
                    hand(3, 1, 2, 3, i)
                else:
                    hand(2, 1, 3, 4, i)

            rows_out(k, i)
        else:
            z_wait(3, i)
            rows_out(k, i)

    def early(i):
        @pl.when(inner)
        def _():
            if i == 2:
                out_push(1)
            rows_out(3, i)

    def late(i):
        @pl.when(jnp.logical_not(inner))
        def _():
            z_piece(3, i)
            if i == 2:
                out_push(1)

    def x_piece(k, i):
        c0, n = spans()[i]
        arrived(comp_v.at[pl.ds(row0(k, 1), cap), pl.ds(c0, n)], x_send.at[k, i], x_recv.at[k, i])
        if i == 0:
            near_push(k, 1)

    def span(u):
        if u < 3:
            return pair_row(u), X_SIDE * cap
        return row0(3, u - 3), cap

    def part_ref(u, s):
        r, n = (row0(0, 1), cap) if u == 0 else span(u)
        return comp_v.at[pl.ds(r, n), pl.ds(col(s), part)]

    def y_arrive(u):
        k = min(u, 3)
        for j in (0, 1) if 0 < u < 3 else (1,) if u == 0 else (u - 3,):
            arrived(near_ref(k, j, ty), y_send.at[k, j], y_recv.at[k, j])
        for i, s in enumerate((t, ty)):
            push(part_ref(u, s), part_ref(u, s), c_send.at[u, i], c_recv.at[u, i], e, tc)

    def core_arrive(u):
        for i, s in enumerate((tc, tyc)):
            arrived(part_ref(u, s), c_send.at[u, i], c_recv.at[u, i])

    def hid_ref(u, s):
        r, n = span(u)
        return hid_v.at[pl.ds(r, n), pl.ds(pl.multiple_of(s * hid, 128), hid)]

    def expert_in(u):
        r, n = span(u)
        rows = comp_v[pl.ds(r, n), :]
        g = jnp.dot(rows, gate_v[...], preferred_element_type=f32)
        u_val = jnp.dot(rows, up_v[...], preferred_element_type=f32)
        hid_ref(u, t)[...] = (g / (1.0 + jnp.exp(-g)) * u_val).astype(bf16)
        push(hid_ref(u, t), hid_ref(u, t), h_send.at[u, 0], h_recv.at[u, 0], e, ty)
        push(hid_ref(u, t), hid_ref(u, t), h_send.at[u, 1], h_recv.at[u, 1], e, tc)

    def hid_forward(u):
        arrived(hid_ref(u, ty), h_send.at[u, 0], h_recv.at[u, 0])
        push(hid_ref(u, ty), hid_ref(u, ty), h_send.at[u, 2], h_recv.at[u, 2], e, tc)

    half = part // 2

    def half_copy(k, h):
        cols = pl.ds(h * half, half)
        return remote(outx_v.at[k, :, cols], pair_v.at[k, pl.ds(cap, cap), cols], rx_send.at[k, h],
                      rx_recv.at[k, h], ex, t)

    def half_push(k, h):
        go = start if k != 1 else lambda cp: cp.start()
        go(half_copy(k, h))

    def hid_wait(u):
        arrived(hid_ref(u, tc), h_send.at[u, 1], h_recv.at[u, 1])
        arrived(hid_ref(u, tyc), h_send.at[u, 2], h_recv.at[u, 2])

    def out_push(k):
        half_push(k, 0)
        half_push(k, 1)

    def expert_out(k, send=True):
        if k < 3:
            hid_wait(k)
        for j in (1, 0):
            if k == 3:
                hid_wait(3 + j)
            rows = hid_v[pl.ds(row0(k, j), cap), :]
            for q in range(part // 256):
                o = jnp.dot(rows, down_v[:, q * 256:(q + 1) * 256], preferred_element_type=f32).astype(bf16)
                if j:
                    outx_v[k, :, q * 256:(q + 1) * 256] = o
                    if send and (q + 1) * 256 % half == 0:
                        half_push(k, (q + 1) * 256 // half - 1)
                else:
                    pair_v[k, :cap, q * 256:(q + 1) * 256] = o

    def rz_copy(k, h):
        cols = pl.ds(h * half, half)
        return remote(part_send.at[k, :, cols], part_z.at[turn[k], :, cols], rz_send.at[k, h],
                      rz_recv.at[turn[k], h], zs[k] * X_SIDE + x, t)

    def sum_when(k, here):
        @pl.when(here)
        def _():
            sum_x(k)

    def sum_x(k):
        for h in (0, 1):
            cols = pl.ds(h * half, half)
            arrived(pair_v.at[k, pl.ds(cap, cap), cols], rx_send.at[k, h], rx_recv.at[k, h])
            both = jnp.dot(mixw_v[turn[k]], pair_v[k, :, cols], preferred_element_type=f32)
            if k:
                part_send[k, :, cols] = both.astype(bf16)
                go = start if k == 3 else lambda cp: cp.start()
                go(rz_copy(k, h))
            else:
                acc_v[:, cols] = both

    def shared():
        loads["sg"].wait()
        loads["su"].wait()
        rows = raw_v[pl.ds(own, toks), :]
        g = jnp.dot(rows, sg_v[...], preferred_element_type=f32)
        u = jnp.dot(rows, su_v[...], preferred_element_type=f32)
        shared_hidden = (g / (1.0 + jnp.exp(-g)) * u).astype(bf16)
        loads["sd"].wait()
        for q in range(width // 512):
            sh_v[:, q * 512:(q + 1) * 512] = jnp.dot(
                shared_hidden, sd_v[:, q * 512:(q + 1) * 512], preferred_element_type=f32).astype(bf16)
        for i, s in enumerate((tc, tyc)):
            push(sh_v.at[:, pl.ds(col(s), part)], sh_core.at[i], m_send.at[0, i], m_recv.at[0, i], e, tc)

    def pool():
        @pl.when(e == 0)
        def _():
            halo_v[...] = jnp.zeros_like(halo_v)

        @pl.when(e > 0)
        def _():
            halo_copy(e - 1).wait_recv()

        ext_v[:HALO, :] = halo_v[...].astype(f32)
        ext_v[HALO:, :] = pool_v[...].astype(f32)
        loads["map"].wait()
        loads["scale"].wait()
        dim = map_v.shape[1]
        position = (e * count + lax.broadcasted_iota(jnp.int32, (count, dim), 0)).astype(f32)
        for grp in range(map_v.shape[0]):
            w = windows[grp % 4]
            cs = slice(grp * dim, (grp + 1) * dim)
            values = ext_v[HALO:, cs]
            running = values
            for lag in range(1, w):
                running = running + ext_v[HALO - lag:HALO - lag + count, cs]
            pooled = (running / jnp.minimum(position + 1.0, float(w)) - values).astype(bf16)
            mapped = jnp.dot(pooled, map_v[grp], preferred_element_type=f32)
            group_v[:, cs] = (mapped * scale_v[:, cs]).astype(bf16)

    def proj():
        loads["proj"].wait()

        def proj_step(q, carry):
            cq = pl.ds(pl.multiple_of(q * 512, 512), 512)
            mix_v[:, cq] = jnp.dot(group_v[...], proj_v[:, cq], preferred_element_type=f32).astype(bf16)
            return carry

        lax.fori_loop(0, width // 512, proj_step, 0)
        for i, s in enumerate((tc, tyc)):
            push(mix_v.at[:, pl.ds(col(s), part)], mix_core.at[i], m_send.at[1, i], m_recv.at[1, i], e, tc)

    def core_sum(which, own_ref, core_ref, send_ref):
        for i in (0, 1):
            arrived(core_ref.at[i], m_send.at[which, i], m_recv.at[which, i])
        send_ref[...] = (own_ref[:, pl.ds(col(ty), part)].astype(f32) + core_ref[1].astype(f32)).astype(bf16)

    def sh_core_sum():
        core_sum(0, sh_v, sh_core, sh_send)

    def sh_push():
        push(sh_send, sh_y, m_send.at[0, 2], m_recv.at[0, 2], e, ty)

    def mix_core_sum():
        core_sum(1, mix_v, mix_core, mix_send)

    piece = count // MIX_PARTS

    def mix_push(n):
        push(mix_send.at[pl.ds(n * piece, piece)], mix_y.at[pl.ds(n * piece, piece)], ms_send.at[n], ms_recv.at[n],
             e, ty)

    def mix_final():
        for n in range(MIX_PARTS):
            arrived(mix_y.at[pl.ds(n * piece, piece)], ms_send.at[n], ms_recv.at[n])
        mix_out[...] = (mix_v[:, pl.ds(col(t), part)].astype(f32) + mix_core[0].astype(f32)
                        + mix_y[...].astype(f32)).astype(bf16)

    def sh_final():
        arrived(sh_y, m_send.at[0, 2], m_recv.at[0, 2])
        acc_v[...] = (acc_v[...] + sh_v[:, pl.ds(col(t), part)].astype(f32) + sh_core[0].astype(f32)
                      + sh_y[...].astype(f32))

    def z_final(h):
        cols = pl.ds(h * half, half)
        total = acc_v[:, cols]
        for k in (1, 2, 3):
            arrived(part_z.at[k, :, cols], rz_send.at[k, h], rz_recv.at[k, h])
            total = total + part_z[k, :, cols].astype(f32)
        moe_out[:, cols] = total.astype(bf16)

    def experts_loaded():
        loads["gate"].wait()
        loads["up"].wait()

    outer = jnp.logical_not(inner)
    shared()
    w_arrive(1)
    w_arrive(2)
    w_arrive(3)
    pool()
    sh_core_sum()
    proj()
    x_piece(0, 0)
    z_piece(1, 0)
    near_push(1, 0)
    x_piece(0, 1)
    mix_core_sum()
    z_piece(1, 1)
    x_piece(0, 2)
    y_arrive(0)
    z_piece(1, 2)
    x_piece(1, 0)
    core_arrive(0)
    experts_loaded()
    expert_in(0)
    z_piece(2, 0)
    near_push(2, 0)
    x_piece(1, 1)
    x_piece(1, 2)
    y_arrive(1)
    z_piece(2, 1)
    x_piece(2, 0)
    core_arrive(1)
    expert_in(1)
    hid_forward(0)
    z_piece(2, 2)
    early(0)
    early(1)
    x_piece(2, 1)
    loads["down"].wait()
    expert_out(0, False)
    late(0)
    x_piece(2, 2)
    hid_forward(1)
    near_push(3, 0)
    y_arrive(2)
    late(1)
    expert_out(1, False)
    early(2)
    core_arrive(2)
    x_piece(3, 0)
    expert_in(2)
    late(2)
    y_arrive(3)
    x_piece(3, 1)
    core_arrive(3)
    hid_forward(2)
    sum_when(1, inner)
    expert_in(3)
    expert_out(2)
    x_piece(3, 2)
    y_arrive(4)
    hid_forward(3)
    core_arrive(4)
    expert_in(4)
    sh_push()
    mix_push(0)
    mix_push(1)
    mix_push(2)
    mix_push(3)
    sum_when(1, outer)
    sum_when(2, inner)
    hid_forward(4)
    expert_out(3)
    sum_when(2, outer)
    sum_x(3)
    out_push(0)
    sum_x(0)
    sh_final()
    mix_final()
    z_final(0)
    z_final(1)

    for cp in sent:
        cp.wait_send()
    for i in range(3):
        x_copy(3, i).wait_send()
    for i in (0, 1):
        half_copy(1, i).wait_send()
        rz_copy(1, i).wait_send()
        rz_copy(2, i).wait_send()

    @pl.when(inner)
    def _():
        for which in handed:
            hop(*which).wait_send()

    @pl.when(e < n_ep - 1)
    def _():
        halo_copy(e + 1).wait_send()


NEAR = 4


def per_device_fused(
    pool_input, pool_map, pool_scale, out_proj, moe_input, norm_gain, routes, route_weights,
    expert_gate, expert_up, expert_down, shared_gate, shared_up, shared_down,
):
    f32, bf16 = jnp.float32, jnp.bfloat16
    n_ep = lax.axis_size("ep")
    toks, width = moe_input.shape
    top_count = routes.shape[1]
    count, channels = pool_input.shape
    dim = pool_map.shape[1]
    part = width // lax.axis_size("tp")
    cap = (3 * toks * top_count + 2 * n_ep - 1) // (2 * n_ep)
    dma = pltpu.SemaphoreType.DMA
    return pl.pallas_call(
        fused_kernel,
        out_shape=(pltpu.VMEM((count, part), bf16), pltpu.VMEM((toks, part), bf16)),
        in_specs=[pl.BlockSpec(memory_space=pl.ANY)] * 14,
        out_specs=(pl.BlockSpec(memory_space=pltpu.VMEM), pl.BlockSpec(memory_space=pltpu.VMEM)),
        scratch_shapes=[
            pltpu.VMEM((count, channels), bf16),
            pltpu.VMEM((channels // dim, dim, dim), bf16),
            pltpu.VMEM((1, channels), f32),
            pltpu.VMEM(out_proj.shape, bf16),
            pltpu.VMEM((toks, width), bf16),
            pltpu.VMEM((1, width), f32),
            pltpu.VMEM((top_count, toks), jnp.int32),
            pltpu.VMEM((top_count, toks), f32),
            pltpu.VMEM(expert_gate.shape[1:], bf16),
            pltpu.VMEM(expert_up.shape[1:], bf16),
            pltpu.VMEM(expert_down.shape[1:], bf16),
            pltpu.VMEM(shared_gate.shape, bf16),
            pltpu.VMEM(shared_up.shape, bf16),
            pltpu.VMEM(shared_down.shape, bf16),
            pltpu.VMEM((HALO, channels), bf16),
            pltpu.VMEM((HALO + count, channels), f32),
            pltpu.VMEM((count, channels), bf16),
            pltpu.VMEM((count, width), bf16),
            pltpu.VMEM((2, count, part), bf16),
            pltpu.VMEM((count, part), bf16),
            pltpu.VMEM((count, part), bf16),
            pltpu.VMEM((Z_SIDE * toks, width), bf16),
            pltpu.VMEM((n_ep * cap, width), bf16),
            pltpu.VMEM((Z_SIDE * cap, width), bf16),
            pltpu.VMEM((Z_SIDE, n_ep, toks), f32),
            pltpu.VMEM((Z_SIDE, n_ep, toks), f32),
            pltpu.VMEM((Z_SIDE, X_SIDE * cap, toks), bf16),
            pltpu.VMEM((Z_SIDE, toks, X_SIDE * cap), bf16),
            pltpu.VMEM((n_ep * cap, expert_down.shape[1]), bf16),
            pltpu.VMEM((Z_SIDE, cap, part), bf16),
            pltpu.VMEM((Z_SIDE, X_SIDE * cap, part), bf16),
            pltpu.VMEM((toks, part), f32),
            pltpu.VMEM((Z_SIDE, toks, part), bf16),
            pltpu.VMEM((Z_SIDE, toks, part), bf16),
            pltpu.VMEM((toks, width), bf16),
            pltpu.VMEM((2, toks, part), bf16),
            pltpu.VMEM((toks, part), bf16),
            pltpu.VMEM((toks, part), bf16),
            dma((14,)), dma((2,)),
            dma((5, 3)), dma((5, 3)), dma((4, 3)), dma((4, 3)), dma((4, 2)), dma((4, 2)),
            dma((5, 2)), dma((5, 2)), dma((4,)), dma((4,)), dma((5, 3)), dma((5, 3)),
            dma((4, 2)), dma((4, 2)), dma((4, 2)), dma((4, 2)), dma((2, 3)), dma((2, 3)),
            dma((MIX_PARTS,)), dma((MIX_PARTS,)),
        ],
        compiler_params=pltpu.CompilerParams(
            collective_id=0, has_side_effects=True, vmem_limit_bytes=60 * 1024 * 1024),
    )(
        pool_input, pool_map, pool_scale.reshape(1, -1), out_proj, moe_input, norm_gain.reshape(1, -1),
        routes.T, route_weights.T, expert_gate, expert_up, expert_down, shared_gate, shared_up, shared_down,
    )


def solution(mesh):
    plane = mesh.shape["ep"] == Z_SIDE * X_SIDE and mesh.shape["tp"] == Y_SIDE * CORES
    body = per_device_fused if plane else per_device
    return jax.shard_map(
        body,
        mesh=mesh,
        in_specs=(
            P("ep", "tp"),
            P(),
            P(),
            P("tp", None),
            P("ep", None),
            P(),
            P("ep", None),
            P("ep", None),
            P("ep", None, "tp"),
            P("ep", None, "tp"),
            P("ep", None, "tp"),
            P(None, "tp"),
            P(None, "tp"),
            P("tp", None),
        ),
        out_specs=(P("ep", "tp"), P("ep", "tp")),
        check_vma=False,
    )
```

```python
import jax
import jax.numpy as jnp
from jax import lax
from jax.experimental import pallas as pl
from jax.experimental.pallas import tpu as pltpu
from jax.sharding import PartitionSpec as P

windows = (2, 4, 8, 16)
reach_back = 15
eps = 1e-05


def passed_along(block, axis, distance):
    devices = range(lax.axis_size(axis))
    route = [(i - distance, i) for i in devices if i - distance in devices]
    return lax.ppermute(block, axis, route)


def pool_branch(pool_input, pool_map, pool_scale, out_proj):
    row_count = pool_input.shape[0]
    channels = pool_input.shape[1]
    group_dim = pool_map.shape[1]
    local_groups = channels // group_dim
    tp_rank = lax.axis_index("tp")
    ep_rank = lax.axis_index("ep")
    earlier_rows = passed_along(pool_input[row_count - reach_back :], "ep", 1)
    values = pool_input.astype(jnp.float32)
    extended = jnp.concatenate([earlier_rows.astype(jnp.float32), values], axis=0)
    position = (ep_rank * row_count + jnp.arange(row_count, dtype=jnp.int32)).astype(jnp.float32)
    group_ids = tp_rank * local_groups + jnp.arange(channels, dtype=jnp.int32) // group_dim
    group_kind = group_ids % 4
    running = jnp.zeros((row_count, channels), jnp.float32)
    pooled = -values
    for lag_step in range(reach_back + 1):
        running = running + extended[reach_back - lag_step : reach_back - lag_step + row_count]
        if lag_step + 1 in windows:
            kind_id = windows.index(lag_step + 1)
            counts = jnp.minimum(position + 1.0, float(lag_step + 1))
            select = (group_kind == kind_id).astype(jnp.float32)
            pooled = pooled + select[None, :] * running / counts[:, None]
    pooled = pooled.astype(jnp.bfloat16)
    my_maps = lax.dynamic_slice_in_dim(pool_map, tp_rank * local_groups, local_groups, 0)
    my_scale = lax.dynamic_slice_in_dim(pool_scale, tp_rank * channels, channels, 0)
    mapped = jnp.einsum(
        "rgc,gcd->rgd",
        pooled.reshape(row_count, local_groups, group_dim),
        my_maps,
        preferred_element_type=jnp.float32,
    )
    group_out = (mapped.reshape(row_count, channels) * my_scale[None, :]).astype(jnp.bfloat16)
    return jnp.dot(group_out, out_proj, preferred_element_type=jnp.float32)


def dispatch_rows(routes, expert_count, capacity):
    tok_count, top_count = routes.shape
    flat_ids = routes.reshape(tok_count * top_count)
    one_hot = (flat_ids[:, None] == jnp.arange(expert_count, dtype=jnp.int32)[None, :]).astype(
        jnp.int32
    )
    earlier = jnp.cumsum(one_hot, axis=0) - one_hot
    slot_ids = jnp.sum(earlier * one_hot, axis=1)
    return (flat_ids * capacity + slot_ids).reshape(tok_count, top_count)


def per_device(
    pool_input,
    pool_map,
    pool_scale,
    out_proj,
    moe_input,
    norm_gain,
    routes,
    route_weights,
    expert_gate,
    expert_up,
    expert_down,
    shared_gate,
    shared_up,
    shared_down,
):
    mixer_part = pool_branch(pool_input, pool_map, pool_scale, out_proj)
    values = moe_input.astype(jnp.float32)
    centre = values - jnp.mean(values, axis=1, keepdims=True)
    variance = jnp.mean(centre * centre, axis=1, keepdims=True)
    normed = (centre * lax.rsqrt(variance + eps) * norm_gain[None, :]).astype(jnp.bfloat16)
    expert_count = lax.axis_size("ep")
    tok_count = moe_input.shape[0]
    top_count = routes.shape[1]
    capacity = (3 * tok_count * top_count + 2 * expert_count - 1) // (2 * expert_count)
    slot_index = dispatch_rows(routes, expert_count, capacity)
    buffer_len = expert_count * capacity
    targets = jnp.arange(buffer_len, dtype=jnp.int32)[:, None]
    placing = jnp.zeros((buffer_len, tok_count), jnp.float32)
    for top_step in range(top_count):
        placing = placing + (targets == slot_index[None, :, top_step]).astype(jnp.float32)
    outgoing = jnp.dot(
        placing.astype(jnp.bfloat16), normed, preferred_element_type=jnp.float32
    ).astype(jnp.bfloat16)
    gate_weight = expert_gate[0]
    up_weight = expert_up[0]
    down_weight = expert_down[0]
    tp_rank = lax.axis_index("tp")
    slice_width = outgoing.shape[1] // lax.axis_size("tp")
    my_slice = lax.dynamic_slice_in_dim(outgoing, tp_rank * slice_width, slice_width, 1)
    arrived = lax.all_to_all(my_slice, "ep", split_axis=0, concat_axis=0, tiled=True)
    shard_cols = lax.all_gather(arrived, "tp", axis=1, tiled=True)
    gate_val = jnp.dot(shard_cols, gate_weight, preferred_element_type=jnp.float32)
    up_val = jnp.dot(shard_cols, up_weight, preferred_element_type=jnp.float32)
    hidden = (jax.nn.silu(gate_val) * up_val).astype(jnp.bfloat16)
    expert_result = jnp.dot(
        lax.all_gather(hidden, "tp", axis=1, tiled=True),
        down_weight,
        preferred_element_type=jnp.float32,
    ).astype(jnp.bfloat16)
    returned = lax.all_to_all(expert_result, "ep", split_axis=0, concat_axis=0, tiled=True)
    routed = jnp.zeros((tok_count, returned.shape[1]), jnp.float32)
    for top_step in range(top_count):
        picked = returned[slot_index[:, top_step]].astype(jnp.float32)
        routed = routed + route_weights[:, top_step, None] * picked
    shared_gate_val = jnp.dot(normed, shared_gate, preferred_element_type=jnp.float32)
    shared_up_val = jnp.dot(normed, shared_up, preferred_element_type=jnp.float32)
    shared_hidden = (jax.nn.silu(shared_gate_val) * shared_up_val).astype(jnp.bfloat16)
    shared_part = jnp.dot(shared_hidden, shared_down, preferred_element_type=jnp.float32)
    mixer_sum, shared_sum = (
        lax.psum_scatter(
            mixer_part.astype(jnp.bfloat16), "tp", scatter_dimension=1, tiled=True
        ).astype(jnp.float32),
        lax.psum_scatter(
            shared_part.astype(jnp.bfloat16), "tp", scatter_dimension=1, tiled=True
        ).astype(jnp.float32),
    )
    return (mixer_sum.astype(jnp.bfloat16), (routed + shared_sum).astype(jnp.bfloat16))


HALO = 16
Z_SIDE, X_SIDE, Y_SIDE, CORES = 4, 2, 2, 2
MIX_PARTS = 4


def fused_kernel(
    pool_h, map_h, scale_h, proj_h, moe_h, gain_h, route_h, rw_h, gate_h, up_h, down_h, sg_h, su_h, sd_h,
    mix_out, moe_out,
    pool_v, map_v, scale_v, proj_v, moe_v, gain_v, route_v, rw_v, gate_v, up_v, down_v, sg_v, su_v, sd_v,
    halo_v, ext_v, group_v, mix_v, mix_core, mix_y, mix_send,
    raw_v, comp_v, xs_v, wts_v, slot_v, pick_v, mixw_v, hid_v, outx_v, pair_v, acc_v, part_z, part_send,
    sh_v, sh_core, sh_y, sh_send,
    load_sem, halo_sem, z_send, z_recv, x_send, x_recv, y_send, y_recv, c_send, c_recv,
    w_send, w_recv, h_send, h_recv, rx_send, rx_recv, rz_send, rz_recv, m_send, m_recv, ms_send, ms_recv,
):
    f32, bf16 = jnp.float32, jnp.bfloat16
    e = lax.axis_index("ep")
    t = lax.axis_index("tp")
    n_ep = Z_SIDE * X_SIDE
    z, x = e // X_SIDE, e % X_SIDE
    y, c = t // CORES, t % CORES
    toks = moe_h.shape[0]
    width = moe_h.shape[1]
    cap = comp_v.shape[0] // n_ep
    part = width // (Y_SIDE * CORES)
    hid = gate_h.shape[2]
    near = NEAR * part // 8
    rest = part - near
    inner = (z > 0) & (z < Z_SIDE - 1)
    kin = [z, z + 1 - 2 * (z % 2), (z + 2) % 4, 3 - z]
    turn = [0, jnp.where(inner, 3, 1), 2, jnp.where(inner, 1, 3)]
    zs = [z, jnp.where(inner, kin[3], kin[1]), kin[2], jnp.where(inner, kin[1], kin[3])]
    xs = [x, 1 - x]
    ex = z * X_SIDE + xs[1]
    ty, tc, tyc = (1 - y) * CORES + c, y * CORES + 1 - c, (1 - y) * CORES + 1 - c

    barrier = pltpu.get_barrier_semaphore()
    for k in range(Z_SIDE):
        for j in range(X_SIDE):
            if k or j:
                pl.semaphore_signal(barrier, inc=1, device_id={"ep": zs[k] * X_SIDE + xs[j], "tp": t},
                                    device_id_type=pl.DeviceIdType.MESH)
    for peer in (ty, tc):
        pl.semaphore_signal(barrier, inc=1, device_id={"ep": e, "tp": peer},
                            device_id_type=pl.DeviceIdType.MESH)

    def raw_row(k):
        return pl.multiple_of(zs[k] * toks, toks)

    def row0(k, j):
        return pl.multiple_of((zs[k] * X_SIDE + xs[j]) * cap, cap)

    def pair_row(k):
        return pl.multiple_of(zs[k] * X_SIDE * cap, X_SIDE * cap)

    def col(s, shift=0):
        return pl.multiple_of(s * part + shift, 128)

    loads = {}
    for i, (name, src, dst) in enumerate((
        ("moe", moe_h, moe_v), ("gain", gain_h, gain_v),
        ("route", route_h, route_v), ("rw", rw_h, rw_v), ("pool", pool_h, pool_v),
        ("map", map_h.at[pl.ds(t * map_v.shape[0], map_v.shape[0])], map_v),
        ("scale", scale_h.at[:, pl.ds(pl.multiple_of(t * scale_v.shape[1], 128), scale_v.shape[1])], scale_v),
        ("sg", sg_h, sg_v), ("su", su_h, su_v), ("sd", sd_h, sd_v), ("proj", proj_h, proj_v),
        ("gate", gate_h.at[0], gate_v), ("up", up_h.at[0], up_v), ("down", down_h.at[0], down_v),
    )):
        cp = pltpu.make_async_copy(src, dst, load_sem.at[i])
        cp.start()
        loads[name] = cp

    sent = []

    def remote(src, dst, ssem, rsem, ep, tp):
        return pltpu.make_async_remote_copy(src_ref=src, dst_ref=dst, send_sem=ssem, recv_sem=rsem,
                                            device_id={"ep": ep, "tp": tp},
                                            device_id_type=pl.DeviceIdType.MESH)

    def start(cp):
        cp.start()
        sent.append(cp)

    def push(src, dst, ssem, rsem, ep, tp):
        start(remote(src, dst, ssem, rsem, ep, tp))

    def arrived(ref, ssem, rsem):
        pltpu.make_async_remote_copy(src_ref=ref, dst_ref=ref, send_sem=ssem, recv_sem=rsem,
                                     device_id={"ep": e, "tp": tc},
                                     device_id_type=pl.DeviceIdType.MESH).wait_recv()

    def routing(k):
        w = wts_v[k]
        a = lax.broadcasted_iota(jnp.int32, (toks, toks), 0)
        b = lax.broadcasted_iota(jnp.int32, (toks, toks), 1)
        before = jnp.where(a < b, 1.0, 0.0).astype(bf16)
        slot = jnp.dot(jnp.where(w > 0.0, 1.0, 0.0).astype(bf16), before, preferred_element_type=f32)
        slot_v[k] = jnp.where(w > 0.0, slot, -1024.0)
        own_row, other_row = slot_v[k, pl.ds(e, 1), :], slot_v[k, pl.ds(ex, 1), :]
        r = lax.broadcasted_iota(jnp.int32, (X_SIDE * cap, toks), 0).astype(f32)
        place = jnp.where(r < float(cap), jnp.broadcast_to(own_row, r.shape),
                          jnp.broadcast_to(other_row, r.shape) + float(cap))
        pick_v[k] = jnp.where(place == r, 1.0, 0.0).astype(bf16)

        def turned(row):
            return jnp.sum(jnp.where(a == b, jnp.broadcast_to(row, (toks, toks)), 0.0), axis=1, keepdims=True)

        s = lax.broadcasted_iota(jnp.int32, (toks, X_SIDE * cap), 1).astype(f32)
        first = s < float(cap)
        place = jnp.where(first, turned(own_row), turned(other_row) + float(cap))
        value = jnp.where(first, turned(wts_v[k, pl.ds(e, 1), :]), turned(wts_v[k, pl.ds(ex, 1), :]))
        mixw_v[k] = jnp.where(place == s, value, 0.0).astype(bf16)

    loads["moe"].wait()
    loads["gain"].wait()
    own = raw_row(0)

    def norm_step(i, carry):
        r = pl.multiple_of(i * 16, 16)
        v = moe_v[pl.ds(r, 16), :].astype(f32)
        cen = v - jnp.mean(v, axis=1, keepdims=True)
        var = jnp.mean(cen * cen, axis=1, keepdims=True)
        raw_v[pl.ds(own + r, 16), :] = (cen * lax.rsqrt(var + eps) * gain_v[...]).astype(bf16)
        return carry

    lax.fori_loop(0, toks // 16, norm_step, 0, unroll=4)
    loads["pool"].wait()
    loads["route"].wait()
    loads["rw"].wait()
    ids = lax.broadcasted_iota(jnp.int32, (n_ep, toks), 0)
    weights = jnp.zeros((n_ep, toks), f32)
    for top_step in range(route_v.shape[0]):
        named = jnp.broadcast_to(route_v[top_step:top_step + 1, :], (n_ep, toks)) == ids
        weights = weights + jnp.where(named, jnp.broadcast_to(rw_v[top_step:top_step + 1, :], (n_ep, toks)), 0.0)
    wts_v[0] = weights

    pl.semaphore_wait(barrier, n_ep - 1 + 2)

    for k in range(1, Z_SIDE):
        push(wts_v.at[0], wts_v.at[k], w_send.at[k], w_recv.at[k], kin[k] * X_SIDE + x, t)

    count = pool_v.shape[0]
    tail_ref = pool_v.at[pl.ds(count - HALO, HALO), :]

    def halo_copy(target):
        return pltpu.make_async_remote_copy(src_ref=tail_ref, dst_ref=halo_v, send_sem=halo_sem.at[0],
                                            recv_sem=halo_sem.at[1], device_id={"ep": target, "tp": t},
                                            device_id_type=pl.DeviceIdType.MESH)

    @pl.when(e < n_ep - 1)
    def _():
        halo_copy(e + 1).start()

    def spans():
        return ((col(t), near), (col(t, near), rest), (col(ty, near), rest))

    def raw_ref(k, i):
        c0, n = spans()[i]
        return raw_v.at[pl.ds(pl.multiple_of(kin[k] * toks, toks), toks), pl.ds(c0, n)]

    handed = []

    def hop(k, to, at, slot, i):
        return pltpu.make_async_remote_copy(
            src_ref=raw_ref(k, i), dst_ref=raw_ref(k, i), send_sem=z_send.at[slot, i], recv_sem=z_recv.at[at, i],
            device_id={"ep": kin[to] * X_SIDE + x, "tp": t}, device_id_type=pl.DeviceIdType.MESH)

    def hand(k, to, at, slot, i):
        handed.append((k, to, at, slot, i))
        hop(k, to, at, slot, i).start()

    for i in range(3):
        cp = hop(0, 1, 1, 0, i)
        cp.start()
        sent.append(cp)

        @pl.when(inner)
        def _():
            hand(0, 3, 3, 1, i)

    step = 256

    def gather(k, i):
        c0, n = spans()[i]
        for q in range(n // step):
            cq = pl.ds(pl.multiple_of(c0 + q * step, 128), step)
            o = jnp.dot(pick_v[turn[k]], raw_v[pl.ds(raw_row(k), toks), cq], preferred_element_type=f32).astype(bf16)
            comp_v[pl.ds(row0(k, 0), cap), cq] = o[:cap]
            xs_v[k * cap:(k + 1) * cap, cq] = o[cap:]

    def x_copy(k, i):
        c0, n = spans()[i]
        return remote(xs_v.at[k * cap:(k + 1) * cap, pl.ds(c0, n)], comp_v.at[pl.ds(row0(k, 0), cap), pl.ds(c0, n)],
                      x_send.at[k, i], x_recv.at[k, i], ex, t)

    def x_push(k, i):
        start(x_copy(k, i))

    def near_ref(k, j, s):
        return comp_v.at[pl.ds(row0(k, j), cap), pl.ds(col(s), near)]

    def near_copy(k, j):
        return remote(near_ref(k, j, t), near_ref(k, j, t), y_send.at[k, j], y_recv.at[k, j], e, ty)

    def near_push(k, j):
        start(near_copy(k, j))

    routing(0)
    for i in range(3):
        gather(0, i)
        x_push(0, i)

    def gather_rest(c0, n):
        for q in range(n // step):
            cq = pl.ds(pl.multiple_of(c0 + q * step, 128), step)
            comp_v[pl.ds(row0(0, 0), cap), cq] = jnp.dot(
                pick_v[0, :cap], raw_v[pl.ds(own, toks), cq], preferred_element_type=f32).astype(bf16)

    gather_rest(col(ty), near)
    gather_rest(col(tc), part)
    gather_rest(col(tyc), part)

    def z_wait(k, i):
        arrived(raw_ref(k, i), z_send.at[k, i], z_recv.at[k, i])

    def w_arrive(k):
        arrived(wts_v.at[k], w_send.at[k], w_recv.at[k])
        routing(k)

    def rows_out(k, i):
        go = start if k < 3 else lambda cp: cp.start()
        gather(k, i)
        go(x_copy(k, i))

    def z_piece(k, i):
        if k < 3:
            z_wait(k, i)

            @pl.when(inner)
            def _():
                if k == 1:
                    hand(1, 3, 2, 2, i)
                    z_wait(3, i)
                    hand(3, 1, 2, 3, i)
                else:
                    hand(2, 1, 3, 4, i)

            rows_out(k, i)
        else:
            z_wait(3, i)
            rows_out(k, i)

    def early(i):
        @pl.when(inner)
        def _():
            if i == 2:
                out_push(1)
            rows_out(3, i)

    def late(i):
        @pl.when(jnp.logical_not(inner))
        def _():
            z_piece(3, i)
            if i == 2:
                out_push(1)

    def x_piece(k, i):
        c0, n = spans()[i]
        arrived(comp_v.at[pl.ds(row0(k, 1), cap), pl.ds(c0, n)], x_send.at[k, i], x_recv.at[k, i])
        if i == 0:
            near_push(k, 1)

    def span(u):
        if u < 3:
            return pair_row(u), X_SIDE * cap
        return row0(3, u - 3), cap

    def part_ref(u, s):
        r, n = (row0(0, 1), cap) if u == 0 else span(u)
        return comp_v.at[pl.ds(r, n), pl.ds(col(s), part)]

    def y_arrive(u):
        k = min(u, 3)
        for j in (0, 1) if 0 < u < 3 else (1,) if u == 0 else (u - 3,):
            arrived(near_ref(k, j, ty), y_send.at[k, j], y_recv.at[k, j])
        for i, s in enumerate((t, ty)):
            push(part_ref(u, s), part_ref(u, s), c_send.at[u, i], c_recv.at[u, i], e, tc)

    def core_arrive(u):
        for i, s in enumerate((tc, tyc)):
            arrived(part_ref(u, s), c_send.at[u, i], c_recv.at[u, i])

    def hid_ref(u, s):
        r, n = span(u)
        return hid_v.at[pl.ds(r, n), pl.ds(pl.multiple_of(s * hid, 128), hid)]

    def expert_in(u):
        r, n = span(u)
        rows = comp_v[pl.ds(r, n), :]
        g = jnp.dot(rows, gate_v[...], preferred_element_type=f32)
        u_val = jnp.dot(rows, up_v[...], preferred_element_type=f32)
        hid_ref(u, t)[...] = (g / (1.0 + jnp.exp(-g)) * u_val).astype(bf16)
        push(hid_ref(u, t), hid_ref(u, t), h_send.at[u, 0], h_recv.at[u, 0], e, ty)
        push(hid_ref(u, t), hid_ref(u, t), h_send.at[u, 1], h_recv.at[u, 1], e, tc)

    def hid_forward(u):
        arrived(hid_ref(u, ty), h_send.at[u, 0], h_recv.at[u, 0])
        push(hid_ref(u, ty), hid_ref(u, ty), h_send.at[u, 2], h_recv.at[u, 2], e, tc)

    half = part // 2

    def half_copy(k, h):
        cols = pl.ds(h * half, half)
        return remote(outx_v.at[k, :, cols], pair_v.at[k, pl.ds(cap, cap), cols], rx_send.at[k, h],
                      rx_recv.at[k, h], ex, t)

    def half_push(k, h):
        go = start if k != 1 else lambda cp: cp.start()
        go(half_copy(k, h))

    def hid_wait(u):
        arrived(hid_ref(u, tc), h_send.at[u, 1], h_recv.at[u, 1])
        arrived(hid_ref(u, tyc), h_send.at[u, 2], h_recv.at[u, 2])

    def out_push(k):
        half_push(k, 0)
        half_push(k, 1)

    def expert_out(k, send=True):
        if k < 3:
            hid_wait(k)
        for j in (1, 0):
            if k == 3:
                hid_wait(3 + j)
            rows = hid_v[pl.ds(row0(k, j), cap), :]
            for q in range(part // 256):
                o = jnp.dot(rows, down_v[:, q * 256:(q + 1) * 256], preferred_element_type=f32).astype(bf16)
                if j:
                    outx_v[k, :, q * 256:(q + 1) * 256] = o
                    if send and (q + 1) * 256 % half == 0:
                        half_push(k, (q + 1) * 256 // half - 1)
                else:
                    pair_v[k, :cap, q * 256:(q + 1) * 256] = o

    def rz_copy(k, h):
        cols = pl.ds(h * half, half)
        return remote(part_send.at[k, :, cols], part_z.at[turn[k], :, cols], rz_send.at[k, h],
                      rz_recv.at[turn[k], h], zs[k] * X_SIDE + x, t)

    def sum_when(k, here):
        @pl.when(here)
        def _():
            sum_x(k)

    def sum_x(k):
        for h in (0, 1):
            cols = pl.ds(h * half, half)
            arrived(pair_v.at[k, pl.ds(cap, cap), cols], rx_send.at[k, h], rx_recv.at[k, h])
            both = jnp.dot(mixw_v[turn[k]], pair_v[k, :, cols], preferred_element_type=f32)
            if k:
                part_send[k, :, cols] = both.astype(bf16)
                go = start if k == 3 else lambda cp: cp.start()
                go(rz_copy(k, h))
            else:
                acc_v[:, cols] = both

    def shared():
        loads["sg"].wait()
        loads["su"].wait()
        rows = raw_v[pl.ds(own, toks), :]
        g = jnp.dot(rows, sg_v[...], preferred_element_type=f32)
        u = jnp.dot(rows, su_v[...], preferred_element_type=f32)
        shared_hidden = (g / (1.0 + jnp.exp(-g)) * u).astype(bf16)
        loads["sd"].wait()
        for q in range(width // 512):
            sh_v[:, q * 512:(q + 1) * 512] = jnp.dot(
                shared_hidden, sd_v[:, q * 512:(q + 1) * 512], preferred_element_type=f32).astype(bf16)
        for i, s in enumerate((tc, tyc)):
            push(sh_v.at[:, pl.ds(col(s), part)], sh_core.at[i], m_send.at[0, i], m_recv.at[0, i], e, tc)

    def pool():
        @pl.when(e == 0)
        def _():
            halo_v[...] = jnp.zeros_like(halo_v)

        @pl.when(e > 0)
        def _():
            halo_copy(e - 1).wait_recv()

        ext_v[:HALO, :] = halo_v[...].astype(f32)
        ext_v[HALO:, :] = pool_v[...].astype(f32)
        loads["map"].wait()
        loads["scale"].wait()
        dim = map_v.shape[1]
        position = (e * count + lax.broadcasted_iota(jnp.int32, (count, dim), 0)).astype(f32)
        for grp in range(map_v.shape[0]):
            w = windows[grp % 4]
            cs = slice(grp * dim, (grp + 1) * dim)
            values = ext_v[HALO:, cs]
            running = values
            for lag in range(1, w):
                running = running + ext_v[HALO - lag:HALO - lag + count, cs]
            pooled = (running / jnp.minimum(position + 1.0, float(w)) - values).astype(bf16)
            mapped = jnp.dot(pooled, map_v[grp], preferred_element_type=f32)
            group_v[:, cs] = (mapped * scale_v[:, cs]).astype(bf16)

    def proj():
        loads["proj"].wait()

        def proj_step(q, carry):
            cq = pl.ds(pl.multiple_of(q * 512, 512), 512)
            mix_v[:, cq] = jnp.dot(group_v[...], proj_v[:, cq], preferred_element_type=f32).astype(bf16)
            return carry

        lax.fori_loop(0, width // 512, proj_step, 0)
        for i, s in enumerate((tc, tyc)):
            push(mix_v.at[:, pl.ds(col(s), part)], mix_core.at[i], m_send.at[1, i], m_recv.at[1, i], e, tc)

    def core_sum(which, own_ref, core_ref, send_ref):
        for i in (0, 1):
            arrived(core_ref.at[i], m_send.at[which, i], m_recv.at[which, i])
        send_ref[...] = (own_ref[:, pl.ds(col(ty), part)].astype(f32) + core_ref[1].astype(f32)).astype(bf16)

    def sh_core_sum():
        core_sum(0, sh_v, sh_core, sh_send)

    def sh_push():
        push(sh_send, sh_y, m_send.at[0, 2], m_recv.at[0, 2], e, ty)

    def mix_core_sum():
        core_sum(1, mix_v, mix_core, mix_send)

    piece = count // MIX_PARTS

    def mix_push(n):
        push(mix_send.at[pl.ds(n * piece, piece)], mix_y.at[pl.ds(n * piece, piece)], ms_send.at[n], ms_recv.at[n],
             e, ty)

    def mix_final():
        for n in range(MIX_PARTS):
            arrived(mix_y.at[pl.ds(n * piece, piece)], ms_send.at[n], ms_recv.at[n])
        mix_out[...] = (mix_v[:, pl.ds(col(t), part)].astype(f32) + mix_core[0].astype(f32)
                        + mix_y[...].astype(f32)).astype(bf16)

    def sh_final():
        arrived(sh_y, m_send.at[0, 2], m_recv.at[0, 2])
        acc_v[...] = (acc_v[...] + sh_v[:, pl.ds(col(t), part)].astype(f32) + sh_core[0].astype(f32)
                      + sh_y[...].astype(f32))

    def z_final(h):
        cols = pl.ds(h * half, half)
        total = acc_v[:, cols]
        for k in (1, 2, 3):
            arrived(part_z.at[k, :, cols], rz_send.at[k, h], rz_recv.at[k, h])
            total = total + part_z[k, :, cols].astype(f32)
        moe_out[:, cols] = total.astype(bf16)

    def experts_loaded():
        loads["gate"].wait()
        loads["up"].wait()

    outer = jnp.logical_not(inner)
    shared()
    w_arrive(1)
    w_arrive(2)
    w_arrive(3)
    pool()
    sh_core_sum()
    proj()
    x_piece(0, 0)
    z_piece(1, 0)
    near_push(1, 0)
    x_piece(0, 1)
    mix_core_sum()
    z_piece(1, 1)
    x_piece(0, 2)
    y_arrive(0)
    z_piece(1, 2)
    x_piece(1, 0)
    core_arrive(0)
    experts_loaded()
    expert_in(0)
    z_piece(2, 0)
    near_push(2, 0)
    x_piece(1, 1)
    x_piece(1, 2)
    y_arrive(1)
    z_piece(2, 1)
    x_piece(2, 0)
    core_arrive(1)
    expert_in(1)
    hid_forward(0)
    z_piece(2, 2)
    early(0)
    early(1)
    x_piece(2, 1)
    loads["down"].wait()
    expert_out(0, False)
    late(0)
    x_piece(2, 2)
    hid_forward(1)
    near_push(3, 0)
    y_arrive(2)
    late(1)
    expert_out(1, False)
    early(2)
    core_arrive(2)
    x_piece(3, 0)
    expert_in(2)
    late(2)
    y_arrive(3)
    x_piece(3, 1)
    core_arrive(3)
    mix_push(0)
    hid_forward(2)
    sum_when(1, inner)
    expert_in(3)
    expert_out(2)
    x_piece(3, 2)
    y_arrive(4)
    hid_forward(3)
    core_arrive(4)
    expert_in(4)
    sh_push()
    mix_push(1)
    mix_push(2)
    mix_push(3)
    sum_when(1, outer)
    sum_when(2, inner)
    hid_forward(4)
    expert_out(3)
    sum_when(2, outer)
    sum_x(3)
    out_push(0)
    sum_x(0)
    sh_final()
    mix_final()
    z_final(0)
    z_final(1)

    for cp in sent:
        cp.wait_send()
    for i in range(3):
        x_copy(3, i).wait_send()
    for i in (0, 1):
        half_copy(1, i).wait_send()
        rz_copy(1, i).wait_send()
        rz_copy(2, i).wait_send()

    @pl.when(inner)
    def _():
        for which in handed:
            hop(*which).wait_send()

    @pl.when(e < n_ep - 1)
    def _():
        halo_copy(e + 1).wait_send()


NEAR = 4


def per_device_fused(
    pool_input, pool_map, pool_scale, out_proj, moe_input, norm_gain, routes, route_weights,
    expert_gate, expert_up, expert_down, shared_gate, shared_up, shared_down,
):
    f32, bf16 = jnp.float32, jnp.bfloat16
    n_ep = lax.axis_size("ep")
    toks, width = moe_input.shape
    top_count = routes.shape[1]
    count, channels = pool_input.shape
    dim = pool_map.shape[1]
    part = width // lax.axis_size("tp")
    cap = (3 * toks * top_count + 2 * n_ep - 1) // (2 * n_ep)
    dma = pltpu.SemaphoreType.DMA
    return pl.pallas_call(
        fused_kernel,
        out_shape=(pltpu.VMEM((count, part), bf16), pltpu.VMEM((toks, part), bf16)),
        in_specs=[pl.BlockSpec(memory_space=pl.ANY)] * 14,
        out_specs=(pl.BlockSpec(memory_space=pltpu.VMEM), pl.BlockSpec(memory_space=pltpu.VMEM)),
        scratch_shapes=[
            pltpu.VMEM((count, channels), bf16),
            pltpu.VMEM((channels // dim, dim, dim), bf16),
            pltpu.VMEM((1, channels), f32),
            pltpu.VMEM(out_proj.shape, bf16),
            pltpu.VMEM((toks, width), bf16),
            pltpu.VMEM((1, width), f32),
            pltpu.VMEM((top_count, toks), jnp.int32),
            pltpu.VMEM((top_count, toks), f32),
            pltpu.VMEM(expert_gate.shape[1:], bf16),
            pltpu.VMEM(expert_up.shape[1:], bf16),
            pltpu.VMEM(expert_down.shape[1:], bf16),
            pltpu.VMEM(shared_gate.shape, bf16),
            pltpu.VMEM(shared_up.shape, bf16),
            pltpu.VMEM(shared_down.shape, bf16),
            pltpu.VMEM((HALO, channels), bf16),
            pltpu.VMEM((HALO + count, channels), f32),
            pltpu.VMEM((count, channels), bf16),
            pltpu.VMEM((count, width), bf16),
            pltpu.VMEM((2, count, part), bf16),
            pltpu.VMEM((count, part), bf16),
            pltpu.VMEM((count, part), bf16),
            pltpu.VMEM((Z_SIDE * toks, width), bf16),
            pltpu.VMEM((n_ep * cap, width), bf16),
            pltpu.VMEM((Z_SIDE * cap, width), bf16),
            pltpu.VMEM((Z_SIDE, n_ep, toks), f32),
            pltpu.VMEM((Z_SIDE, n_ep, toks), f32),
            pltpu.VMEM((Z_SIDE, X_SIDE * cap, toks), bf16),
            pltpu.VMEM((Z_SIDE, toks, X_SIDE * cap), bf16),
            pltpu.VMEM((n_ep * cap, expert_down.shape[1]), bf16),
            pltpu.VMEM((Z_SIDE, cap, part), bf16),
            pltpu.VMEM((Z_SIDE, X_SIDE * cap, part), bf16),
            pltpu.VMEM((toks, part), f32),
            pltpu.VMEM((Z_SIDE, toks, part), bf16),
            pltpu.VMEM((Z_SIDE, toks, part), bf16),
            pltpu.VMEM((toks, width), bf16),
            pltpu.VMEM((2, toks, part), bf16),
            pltpu.VMEM((toks, part), bf16),
            pltpu.VMEM((toks, part), bf16),
            dma((14,)), dma((2,)),
            dma((5, 3)), dma((5, 3)), dma((4, 3)), dma((4, 3)), dma((4, 2)), dma((4, 2)),
            dma((5, 2)), dma((5, 2)), dma((4,)), dma((4,)), dma((5, 3)), dma((5, 3)),
            dma((4, 2)), dma((4, 2)), dma((4, 2)), dma((4, 2)), dma((2, 3)), dma((2, 3)),
            dma((MIX_PARTS,)), dma((MIX_PARTS,)),
        ],
        compiler_params=pltpu.CompilerParams(
            collective_id=0, has_side_effects=True, vmem_limit_bytes=60 * 1024 * 1024),
    )(
        pool_input, pool_map, pool_scale.reshape(1, -1), out_proj, moe_input, norm_gain.reshape(1, -1),
        routes.T, route_weights.T, expert_gate, expert_up, expert_down, shared_gate, shared_up, shared_down,
    )


def solution(mesh):
    plane = mesh.shape["ep"] == Z_SIDE * X_SIDE and mesh.shape["tp"] == Y_SIDE * CORES
    body = per_device_fused if plane else per_device
    return jax.shard_map(
        body,
        mesh=mesh,
        in_specs=(
            P("ep", "tp"),
            P(),
            P(),
            P("tp", None),
            P("ep", None),
            P(),
            P("ep", None),
            P("ep", None),
            P("ep", None, "tp"),
            P("ep", None, "tp"),
            P("ep", None, "tp"),
            P(None, "tp"),
            P(None, "tp"),
            P("tp", None),
        ),
        out_specs=(P("ep", "tp"), P("ep", "tp")),
        check_vma=False,
    )
```
